256 devices in a mesh: ep: 32 (over z, x), tp: 8 (over y, core).
Axes of the slice: x: 4, y: 4, z: 8, core: 2. Of those that a mesh axis runs over, the one named last changes fastest.
Arguments:
- tokens: bfloat16 [768, 4096], P('ep'), may hold values from -6 to 6
- delta_state: float32 [768, 16, 128, 128], P('ep', 'tp'), may hold values from -0.625 to 0.625
- attn_gain: float32 [4096], replicated, may hold values from 0.1 to 1.9
- query_weight: bfloat16 [4096, 2048], P('ep', 'tp'), may hold values from -0.09375 to 0.09375
- key_weight: bfloat16 [4096, 2048], P('ep', 'tp'), may hold values from -0.09375 to 0.09375
- value_weight: bfloat16 [4096, 2048], P('ep', 'tp'), may hold values from -0.09375 to 0.09375
- decay_weight: bfloat16 [4096, 16], replicated, may hold values from -0.09375 to 0.09375
- beta_weight: bfloat16 [4096, 16], replicated, may hold values from -0.09375 to 0.09375
- decay_rate: float32 [16], P('tp'), may hold values from 0.05 to 3
- head_gain: float32 [128], replicated, may hold values from 0.1 to 1.9
- output_weight: bfloat16 [2048, 4096], P('tp'), may hold values from -0.125 to 0.125
- ffn_gain: float32 [4096], replicated, may hold values from 0.1 to 1.9
- expert_ids: int32 [768, 2], P('ep'), may hold values from 0 to 31, all different within a row; in each aligned block of 24 rows (0 to 23, 24 to 47, ...) at most 3 rows name the same one
- group_prob: float32 [768], P('ep'), may hold values from 0.3 to 1
- expert_logit: float32 [768, 2], P('ep'), may hold values from -8 to 8
- expert_gate: bfloat16 [32, 4096, 1024], P('ep', None, 'tp'), may hold values from -0.09375 to 0.09375
- expert_up: bfloat16 [32, 4096, 1024], P('ep', None, 'tp'), may hold values from -0.09375 to 0.09375
- expert_down: bfloat16 [32, 1024, 4096], P('ep', 'tp'), may hold values from -0.1875 to 0.1875
- dense_gate: bfloat16 [4096, 4096], P('tp', 'ep'), may hold values from -0.09375 to 0.09375
- dense_up: bfloat16 [4096, 4096], P('tp', 'ep'), may hold values from -0.09375 to 0.09375
- dense_down: bfloat16 [4096, 4096], P('ep', 'tp'), may hold values from -0.09375 to 0.09375
- dense_mix: float32 [4096], P('tp'), may hold values from -3 to 3
Outputs:
- mixed_out: bfloat16 [768, 4096], P('ep', 'tp')
- new_state: float32 [768, 16, 128, 128], P('ep', 'tp')
The draws below stay inside these ranges and needn't reach their ends.
Inputs may be any that keep to these rules, and one draw needn't show every extreme that they name: `expert_ids`: each row names 2 different experts. Among the rows of one device (aligned blocks of 24 rows) no expert is named by more than 3 rows, and in every draw some expert reaches 3 in some block.
All inputs are finite; a program needn't handle non-finite values.
Results may differ from the reference program's by a relative error of at most 0.02.
Values may be sent and summed in bfloat16 or wider, within the bound.
A program may use at most 64 MiB of HBM per device.

```python
import math
import jax
import jax.numpy as jnp
import numpy as np
from jax import lax

D = 4096
HEADS = 16
HEAD = 128
FE = 1024
FD = 4096
TOPK = 2
SEQ_DEV = 24
BATCH = 768
EXPERTS = 32
CAP = 3
N_EP = 32
N_TP = 8


def block_scale(stream_key, extent, pieces, low, top_value):
    factor_of = 1.0
    for dim, blocks in pieces:
        heights = jax.random.uniform(jax.random.fold_in(jax.random.fold_in(stream_key, 6), dim), (blocks,), jnp.float32, low / len(pieces), top_value / len(pieces))
        factor_of = factor_of * jnp.repeat(jnp.exp(heights), extent[dim] // blocks).reshape((-1,) + (1,) * (len(extent) - 1 - dim))
    return factor_of


def routed_block(own_key, own, number, rows, count, top, reach, slope):
    sequence = jax.random.permutation(own_key, count)
    crowded, usual = portions_of(count, rows * top, reach, slope, True), portions_of(count, rows * top, reach, slope, False)
    places = jnp.arange(count)

    def named(lengths, offset_by):
        used = int((lengths > 0).sum())
        fixed = max(1, used // 4)
        shifted = fixed + (places - fixed + offset_by * (used - fixed)) % max(1, count - fixed)
        return jnp.zeros((count,), jnp.int32).at[sequence[jnp.where(places < fixed, places, shifted)]].set(jnp.asarray(lengths, jnp.int32))

    lengths = jnp.where(number % 4 == 0, named(crowded, number // 4), named(usual, number - number // 4 - 1))
    mixed = jax.random.permutation(jax.random.fold_in(own, 3), count)
    giver, receiver = mixed[0:count // 2 * 2:2], mixed[1:count // 2 * 2:2]
    slack = jnp.minimum(lengths[giver] - 1, reach - lengths[receiver]) // 2
    slack = jnp.where((giver == sequence[0]) | (receiver == sequence[0]) | (lengths[receiver] == 0), 0, jnp.maximum(slack, 0))
    shifted = jax.random.randint(jax.random.fold_in(own, 4), (count // 2,), 0, 1 << 20) % (slack + 1)
    lengths = lengths.at[giver].add(-shifted).at[receiver].add(shifted)
    items = jnp.searchsorted(jnp.cumsum(lengths), jnp.arange(rows * top), side="right").astype(jnp.int32)
    table = items.reshape(top, rows).T
    table = table[jax.random.permutation(jax.random.fold_in(own, 1), rows)]
    offset_by = jax.random.randint(jax.random.fold_in(own, 2), (rows, 1), 0, top)
    return jnp.take_along_axis(table, (jnp.arange(top)[None, :] + offset_by) % top, axis=1)


def portions_of(count, total, most, lean, full):
    portions = [(1 << 20) // math.isqrt(grade ** lean) + 1 for grade in range(1, count + 1)]
    largest = most if full else min(most, max(-(-total // count), total * portions[0] // sum(portions)))
    least = 1 if total - largest >= count - 1 else 0
    holding, rest = [largest] + [least] * (count - 1), total - largest - least * (count - 1)
    while rest > 0:
        free = [i for i in range(1, count) if holding[i] < largest] or [i for i in range(1, count) if holding[i] < most]
        whole, budget = sum([portions[i] for i in free]), rest
        for i in free:
            more = min(most - holding[i], max(1, budget * portions[i] // whole), rest)
            holding[i] = holding[i] + more
            rest = rest - more
    return np.array(holding)


def bell_draw(stream_key, extent, width, most, pieces=(), held_as=jnp.bfloat16):
    drawn = width * jax.random.normal(stream_key, extent, jnp.float32)
    if pieces:
        drawn = drawn * block_scale(stream_key, extent, pieces, -0.22, 0.18)
    return jnp.clip(drawn, -most, most).astype(held_as)


def setup_inputs(seed: int = 0) -> dict:
    keys = jax.random.split(jax.random.key(seed), 23)
    tokens = bell_draw(keys[0], (BATCH, D), 1.0, 6.0, ((0, 32),))
    delta_state = bell_draw(keys[1], (BATCH, HEADS, HEAD, HEAD), 0.1, 0.625, ((0, 32), (1, 8)), jnp.float32)
    attn_gain = jnp.clip(1.0 + 0.18 * jax.random.normal(keys[2], (D,), jnp.float32), 0.1, 1.9)
    query_weight = bell_draw(keys[3], (D, HEADS * HEAD), D ** -0.5, 0.09375, ((0, 32), (1, 8)))
    key_weight = bell_draw(keys[4], (D, HEADS * HEAD), D ** -0.5, 0.09375, ((0, 32), (1, 8)))
    value_weight = bell_draw(keys[5], (D, HEADS * HEAD), D ** -0.5, 0.09375, ((0, 32), (1, 8)))
    decay_weight = bell_draw(keys[6], (D, HEADS), D ** -0.5, 0.09375)
    beta_weight = bell_draw(keys[7], (D, HEADS), D ** -0.5, 0.09375)
    decay_rate = jnp.clip(jnp.exp(math.log(3.0) - 4.0943445 * jax.random.uniform(keys[8], (HEADS,), jnp.float32) ** block_scale(keys[8], (HEADS,), ((0, 8),), -0.2, 0.2)), 0.05, 3.0)
    head_gain = jnp.clip(1.0 + 0.18 * jax.random.normal(keys[9], (HEAD,), jnp.float32), 0.1, 1.9)
    output_weight = bell_draw(keys[10], (HEADS * HEAD, D), (HEADS * HEAD) ** -0.5, 0.125, ((0, 8),))
    ffn_gain = jnp.clip(1.0 + 0.18 * jax.random.normal(keys[11], (D,), jnp.float32), 0.1, 1.9)
    expert_ids_keys = jax.random.split(jax.random.fold_in(keys[12], 1), BATCH // SEQ_DEV)
    expert_ids_turns = jax.random.permutation(jax.random.fold_in(keys[12], 3), BATCH // SEQ_DEV)
    expert_ids = jax.vmap(lambda own, number: routed_block(jax.random.fold_in(keys[12], 2), own, number, SEQ_DEV, EXPERTS, TOPK, CAP, 2))(expert_ids_keys, expert_ids_turns).reshape((BATCH, TOPK))
    group_prob = jnp.clip(0.3 + 0.7 * jax.random.uniform(keys[13], (BATCH,), jnp.float32) ** block_scale(keys[13], (BATCH,), ((0, 32),), -0.2, 0.2), 0.3, 1.0)
    expert_logit = bell_draw(keys[14], (BATCH, TOPK), 1.5, 8.0, ((0, 32),), jnp.float32)
    expert_gate = bell_draw(keys[15], (EXPERTS, D, FE), D ** -0.5, 0.09375, ((0, 32), (2, 8)))
    expert_up = bell_draw(keys[16], (EXPERTS, D, FE), D ** -0.5, 0.09375, ((0, 32), (2, 8)))
    expert_down = bell_draw(keys[17], (EXPERTS, FE, D), FE ** -0.5, 0.1875, ((0, 32), (1, 8)))
    dense_gate = bell_draw(keys[18], (D, FD), D ** -0.5, 0.09375, ((0, 8), (1, 32)))
    dense_up = bell_draw(keys[19], (D, FD), D ** -0.5, 0.09375, ((0, 8), (1, 32)))
    dense_down = bell_draw(keys[20], (FD, D), FD ** -0.5, 0.09375, ((0, 32), (1, 8)))
    dense_mix = jnp.clip(jax.random.uniform(keys[21], (D,), jnp.float32, -3.0, 3.0) * block_scale(keys[21], (D,), ((0, 8),), -0.4, 0.0), -3.0, 3.0)
    return {"tokens": tokens, "delta_state": delta_state, "attn_gain": attn_gain, "query_weight": query_weight, "key_weight": key_weight, "value_weight": value_weight, "decay_weight": decay_weight, "beta_weight": beta_weight, "decay_rate": decay_rate, "head_gain": head_gain, "output_weight": output_weight, "ffn_gain": ffn_gain, "expert_ids": expert_ids, "group_prob": group_prob, "expert_logit": expert_logit, "expert_gate": expert_gate, "expert_up": expert_up, "expert_down": expert_down, "dense_gate": dense_gate, "dense_up": dense_up, "dense_down": dense_down, "dense_mix": dense_mix}


EPS = 1e-06

def rms_scale(values, gain):
    mean_sq = lax.optimization_barrier(jnp.mean(values * values, axis=-1, keepdims=True))
    return values * lax.rsqrt(mean_sq + EPS) * gain

def unit_rows(values):
    return values * lax.rsqrt(lax.optimization_barrier(jnp.sum(values * values, axis=-1, keepdims=True)) + EPS)

def rounded_back(values):
    return lax.optimization_barrier(values.astype(jnp.bfloat16)).astype(jnp.float32)

def block_sum(left, right, blocks):
    size = left.shape[1] // blocks
    total = jnp.zeros((left.shape[0], right.shape[1]), jnp.float32)
    for index in range(blocks):
        part = jnp.dot(left[:, index * size:(index + 1) * size], right[index * size:(index + 1) * size], preferred_element_type=jnp.float32)
        total = total + rounded_back(part)
    return total

def reference(tokens, delta_state, attn_gain, query_weight, key_weight, value_weight, decay_weight, beta_weight, decay_rate, head_gain, output_weight, ffn_gain, expert_ids, group_prob, expert_logit, expert_gate, expert_up, expert_down, dense_gate, dense_up, dense_down, dense_mix):
    residual = tokens.astype(jnp.float32)
    normed = rms_scale(residual, attn_gain).astype(jnp.bfloat16)

    def heads_of(weight):
        product = jnp.dot(normed, weight, preferred_element_type=jnp.float32)
        return rounded_back(product).reshape(BATCH, HEADS, HEAD)
    query_unit = unit_rows(heads_of(query_weight)) * HEAD ** (-0.5)
    key_unit = unit_rows(heads_of(key_weight))
    value_heads = heads_of(value_weight)
    decay = jnp.exp(-decay_rate * jax.nn.softplus(jnp.dot(normed, decay_weight, preferred_element_type=jnp.float32)))
    beta_gate = jax.nn.sigmoid(jnp.dot(normed, beta_weight, preferred_element_type=jnp.float32))
    recalled = jnp.einsum('bhk,bhkv->bhv', key_unit, delta_state, precision=lax.Precision.HIGHEST)
    correction = beta_gate[..., None] * (value_heads - decay[..., None] * recalled)
    new_state = decay[..., None, None] * delta_state + key_unit[..., :, None] * correction[..., None, :]
    read_out = jnp.einsum('bhk,bhkv->bhv', query_unit, new_state, precision=lax.Precision.HIGHEST)
    head_out = rms_scale(read_out, head_gain).astype(jnp.bfloat16).reshape(BATCH, HEADS * HEAD)
    attn_sum = block_sum(head_out, output_weight, N_TP)
    middle = residual + attn_sum
    ffn_in = rms_scale(middle, ffn_gain).astype(jnp.bfloat16)
    dense_pre_gate = block_sum(ffn_in, dense_gate, N_TP)
    dense_pre_up = block_sum(ffn_in, dense_up, N_TP)
    dense_hidden = (jax.nn.silu(dense_pre_gate) * dense_pre_up).astype(jnp.bfloat16)
    dense_out = jnp.dot(dense_hidden, dense_down, preferred_element_type=jnp.float32)
    pairs = SEQ_DEV * TOPK
    block_ids = expert_ids.reshape(N_EP, pairs)
    onehot = (block_ids[:, :, None] == jnp.arange(EXPERTS, dtype=jnp.int32)[None, None, :]).astype(jnp.int32)
    ranks = lax.optimization_barrier(jnp.sum(onehot * (jnp.cumsum(onehot, axis=1) - 1), axis=2))
    sources = jnp.arange(N_EP, dtype=jnp.int32)[:, None]
    places = (block_ids * (N_EP * CAP) + sources * CAP + ranks).reshape(-1).astype(jnp.int32)
    repeated = jnp.repeat(ffn_in, TOPK, axis=0)
    slots = jnp.zeros((EXPERTS * N_EP * CAP, D), jnp.bfloat16).at[places].set(repeated)
    slots = slots.reshape(EXPERTS, N_EP * CAP, D)

    def one_expert(inputs):
        arrived, gate_w, up_w, down_w = inputs
        gate_vals = jnp.dot(arrived, gate_w, preferred_element_type=jnp.float32)
        up_vals = jnp.dot(arrived, up_w, preferred_element_type=jnp.float32)
        expert_hidden = (jax.nn.silu(gate_vals) * up_vals).astype(jnp.bfloat16)
        return block_sum(expert_hidden, down_w, N_TP).astype(jnp.bfloat16)
    expert_result = lax.map(one_expert, (slots, expert_gate, expert_up, expert_down))
    picked = jnp.take(expert_result.reshape(EXPERTS * N_EP * CAP, D), places, axis=0)
    picked = picked.astype(jnp.float32).reshape(BATCH, TOPK, D)
    logit_exp = jnp.exp(expert_logit)
    route_weight = group_prob[:, None] * logit_exp / lax.optimization_barrier(jnp.sum(logit_exp, axis=1, keepdims=True))
    expert_mix = lax.optimization_barrier(jnp.sum(route_weight[..., None] * picked, axis=1))
    mixed_out = (middle + jax.nn.sigmoid(dense_mix) * dense_out + expert_mix).astype(jnp.bfloat16)
    return (mixed_out, new_state)
```

```python
import jax
import jax.numpy as jnp
from jax import lax
from jax.experimental import pallas as pl
from jax.experimental.pallas import tpu as pltpu
from jax.sharding import PartitionSpec as P

EPS = 1e-06
MESH = pl.DeviceIdType.MESH
F32 = jnp.float32
BF16 = jnp.bfloat16

NX, NZ, NT = 4, 8, 8
ROWS = 24
D = 4096
SL = 512
HEAD = 128
CAP = 3
SLOTS = NZ * CAP


def kernel(
    tok_h, state_h, again_h, wq_h, wk_h, wv_h, dT_h, bT_h, rate_s, hgain_h, wo_h, fgain_h, info_h,
    eg_h, eu_h, ed_h, dg_h, du_h, dd_h, mix_h,
    out_ref, state_o,
    tok, tokf, again, wqkv, db, hgain, wo, fgain, info, wgu, wdn, mixv, egu, edn, state,
    spread, act, psrc, pdst, rout, asrc, adst, ssb, xall, dsrc, ddst, hall, esrc, eall, ehall, rsrc, rdst, fsrc, fdst,
    lsem, xs, xr, zs, zr, ts, tr,
):
    ep = lax.axis_index("ep")
    tp = lax.axis_index("tp")
    z = ep // NX
    x = lax.rem(ep, NX)

    def at_x(d):
        return {"ep": z * NX + lax.rem(x + d, NX), "tp": tp}

    def at_z(d):
        return {"ep": lax.rem(z + d, NZ) * NX + x, "tp": tp}

    def at_t(d):
        return {"ep": ep, "tp": lax.rem(tp + d, NT)}

    def remote(src, dst, ss, rs, dev):
        return pltpu.make_async_remote_copy(
            src_ref=src, dst_ref=dst, send_sem=ss, recv_sem=rs, device_id=dev, device_id_type=MESH
        )

    sent = []

    def go(copy):
        copy.start()
        sent.append(copy)
        return copy

    local = []

    def load(src, dst):
        c = pltpu.make_async_copy(src, dst, lsem.at[len(local)])
        c.start()
        local.append(c)
        return c

    l_tok = load(tok_h, tok)
    l_again = load(again_h, again)
    l_w = [load(w, wqkv.at[m, x]) for m, w in enumerate((wk_h, wv_h, wq_h))]
    l_info = load(info_h, info)
    l_db = [load(dT_h, db.at[0]), load(bT_h, db.at[1])]
    l_gu = [load(dg_h, wgu.at[x, :, pl.ds(0, 128)]), load(du_h, wgu.at[x, :, pl.ds(128, 128)])]
    l_dn = load(dd_h, wdn.at[x])
    l_ed = load(ed_h.at[:, pl.ds(pl.multiple_of(tp * SL, SL), SL)], edn.at[tp])
    l_state = load(state_h, state)
    l_wo = load(wo_h, wo)
    l_small = [
        load(hgain_h, hgain),
        load(fgain_h.at[:, pl.ds(pl.multiple_of(tp * SL, SL), SL)], fgain),
        load(mix_h, mixv),
        load(tok_h.at[:, pl.ds(pl.multiple_of(tp * SL, SL), SL)], tokf),
    ]
    l_egu = [load(eg_h, egu.at[:, pl.ds(0, 128)]), load(eu_h, egu.at[:, pl.ds(128, 128)])]

    bar = pltpu.get_barrier_semaphore()
    for d in range(1, NX):
        pl.semaphore_signal(bar, inc=1, device_id=at_x(d), device_id_type=MESH)
    for d in range(1, NZ):
        pl.semaphore_signal(bar, inc=1, device_id=at_z(d), device_id_type=MESH)
    for d in range(1, NT):
        pl.semaphore_signal(bar, inc=1, device_id=at_t(d), device_id_type=MESH)

    l_tok.wait()
    l_again.wait()
    t32 = tok[...].astype(F32)
    ms = jnp.sum(t32 * t32, axis=1, keepdims=True) * (1.0 / D)
    normed = (t32 * lax.rsqrt(ms + EPS) * again[...]).astype(BF16)
    for b in range(NZ):
        spread[b] = normed[:, b * SL : (b + 1) * SL]

    pl.semaphore_wait(bar, NX + NZ + NT - 3)

    nsx = [0]
    nsz = [0]
    nst = [0]

    def nx():
        nsx[0] += 1
        return nsx[0] - 1

    def nz():
        nsz[0] += 1
        return nsz[0] - 1

    def nt():
        nst[0] += 1
        return nst[0] - 1

    left = lax.rem(x + NX - 1, NX)
    right = lax.rem(x + 1, NX)

    def gather_start(buf):
        a, b = nx(), nx()
        c0 = go(remote(buf.at[x], buf.at[x], xs.at[a], xr.at[a], at_x(1)))
        c1 = go(remote(buf.at[x], buf.at[x], xs.at[b], xr.at[b], at_x(NX - 1)))
        return c0, c1

    def gather_relay(buf, c0, c1):
        h = buf.shape[1] // 2
        a, b = nx(), nx()
        c0.wait_recv()
        r0 = go(remote(
            buf.at[left, pl.ds(0, h)], buf.at[left, pl.ds(0, h)], xs.at[a], xr.at[a], at_x(1)))
        c1.wait_recv()
        r1 = go(remote(
            buf.at[right, pl.ds(h, h)], buf.at[right, pl.ds(h, h)], xs.at[b], xr.at[b], at_x(NX - 1)))
        return r0, r1

    for c in l_w:
        c.wait()
    g_w = [gather_start(wqkv.at[m]) for m in range(3)]

    c_spread = []
    for d in range(1, NZ):
        i = nz()
        zd = lax.rem(z + d, NZ)
        c_spread.append(go(remote(spread.at[zd], act.at[z], zs.at[i], zr.at[i], at_z(d))))
    act[z] = spread[z]

    c_ed = []
    for d in range(1, NT):
        i = nt()
        td = lax.rem(tp + d, NT)
        c_ed.append(go(remote(
            ed_h.at[:, pl.ds(pl.multiple_of(td * SL, SL), SL)], edn.at[tp], ts.at[i], tr.at[i], at_t(d))))

    for c in l_db:
        c.wait()
    dims = (((1,), (1,)), ((), ()))
    dpre = lax.dot_general(normed, db[0], dims, preferred_element_type=F32)
    bpre = lax.dot_general(normed, db[1], dims, preferred_element_type=F32)
    lane16 = lax.broadcasted_iota(jnp.int32, dpre.shape, 1)
    decay, beta = [], []
    for h in range(2):
        pick = lane16 == tp * 2 + h
        dp = jnp.sum(jnp.where(pick, dpre, 0.0), axis=1, keepdims=True)
        bp = jnp.sum(jnp.where(pick, bpre, 0.0), axis=1, keepdims=True)
        soft = jnp.maximum(dp, 0.0) + jnp.log(1.0 + jnp.exp(-jnp.abs(dp)))
        decay.append(jnp.exp(-rate_s[h] * soft))
        beta.append(1.0 / (1.0 + jnp.exp(-bp)))

    l_info.wait()
    inf = info[...]
    id0, id1 = inf[:, 0:1], inf[:, 1:2]
    e0, e1 = jnp.exp(inf[:, 2:3]), jnp.exp(inf[:, 3:4])
    den = e0 + e1
    w0, w1 = inf[:, 4:5] * e0 / den, inf[:, 4:5] * e1 / den
    lanef = lax.broadcasted_iota(jnp.int32, (ROWS, 128), 1).astype(F32)
    rowi = lax.broadcasted_iota(jnp.int32, (ROWS, 128), 0)
    oh = jnp.where((lanef == id0) | (lanef == id1), 1.0, 0.0)
    rank = jnp.zeros((ROWS, 128), F32)
    for i in range(ROWS - 1):
        rank = rank + jnp.where(rowi > i, oh[i : i + 1, :], 0.0)
    table = (rank + 1.0) * oh
    for idk, wk in ((id0, w0), (id1, w1)):
        whi = wk.astype(BF16).astype(F32)
        table = table + jnp.where(lanef == idk + 32.0, whi, 0.0)
        table = table + jnp.where(lanef == idk + 64.0, wk - whi, 0.0)
    rout[z] = table.astype(BF16)

    r_w = [gather_relay(wqkv.at[m], *g_w[m]) for m in range(3)]

    for c in c_spread:
        c.wait_recv()
    acts = act[...].reshape(NZ * ROWS, SL)
    c_p = []
    for m in range(3):
        for c in r_w[m]:
            c.wait_recv()
        part = jnp.dot(acts, wqkv[m].reshape(SL, 2 * HEAD), preferred_element_type=F32)
        psrc[m] = part.astype(BF16).reshape(NZ, ROWS, 2 * HEAD)
        row = []
        for d in range(1, NZ):
            i = nz()
            zd = lax.rem(z + d, NZ)
            row.append(go(remote(psrc.at[m, zd], pdst.at[m, z], zs.at[i], zr.at[i], at_z(d))))
        pdst[m, z] = psrc[m, z]
        c_p.append(row)

    c_r = []
    for d in range(1, NZ):
        i = nz()
        c_r.append(go(remote(rout.at[z], rout.at[z], zs.at[i], zr.at[i], at_z(d))))
    for c in l_gu:
        c.wait()
    l_dn.wait()
    g_gu = gather_start(wgu)
    g_dn = gather_start(wdn)

    qkv = []
    for m in range(3):
        for c in c_p[m]:
            c.wait_recv()
        s = pdst[m, 0].astype(F32)
        for b in range(1, NZ):
            s = s + pdst[m, b].astype(F32)
        qkv.append(s.astype(BF16).astype(F32))
    kk, vv, qq = qkv

    l_state.wait()
    for c in l_small:
        c.wait()
    heads = []
    for h in range(2):
        sl = slice(h * HEAD, (h + 1) * HEAD)
        kh, vh, qh = kk[:, sl], vv[:, sl], qq[:, sl]
        ku = kh * lax.rsqrt(jnp.sum(kh * kh, axis=1, keepdims=True) + EPS)
        qu = qh * lax.rsqrt(jnp.sum(qh * qh, axis=1, keepdims=True) + EPS) * HEAD ** (-0.5)
        kT = ku.T
        qT = qu.T
        kq = jnp.sum(ku * qu, axis=1, keepdims=True)
        rec, red = [], []
        for b in range(ROWS):
            st = state[b, h]
            rec.append(jnp.sum(st * kT[:, b : b + 1], axis=0, keepdims=True))
            red.append(jnp.sum(st * qT[:, b : b + 1], axis=0, keepdims=True))
        rec = jnp.concatenate(rec, axis=0)
        red = jnp.concatenate(red, axis=0)
        corr = beta[h] * (vh - decay[h] * rec)
        ro = decay[h] * red + kq * corr
        ro = ro * lax.rsqrt(jnp.mean(ro * ro, axis=1, keepdims=True) + EPS) * hgain[...]
        heads.append(ro.astype(BF16))
        qkv[h] = (kT, corr)

    l_wo.wait()
    hcat = jnp.concatenate(heads, axis=1)
    for t in range(NT):
        asrc[t] = jnp.dot(hcat, wo[:, t * SL : (t + 1) * SL], preferred_element_type=F32).astype(BF16)
    c_a = []
    for d in range(1, NT):
        i = nt()
        td = lax.rem(tp + d, NT)
        c_a.append(go(remote(asrc.at[td], adst.at[tp], ts.at[i], tr.at[i], at_t(d))))
    adst[tp] = asrc[tp]

    for h in range(2):
        kT, corr = qkv[h]
        dcol = decay[h]
        for b in range(ROWS):
            state_o[b, h] = state[b, h] * dcol[b : b + 1, :] + kT[:, b : b + 1] * corr[b : b + 1, :]

    for c in c_a:
        c.wait_recv()
    asum = adst[0].astype(F32)
    for b in range(1, NT):
        asum = asum + adst[b].astype(F32)
    middle = tokf[...].astype(F32) + asum
    ss = jnp.sum(middle * middle, axis=1, keepdims=True)
    eye = lax.broadcasted_iota(jnp.int32, (ROWS, 128), 0) == lax.broadcasted_iota(jnp.int32, (ROWS, 128), 1)
    ssb[tp] = jnp.sum(jnp.where(eye, ss, 0.0), axis=0, keepdims=True)
    c_s = []
    for d in range(1, NT):
        i = nt()
        c_s.append(go(remote(ssb.at[tp], ssb.at[tp], ts.at[i], tr.at[i], at_t(d))))
    r_gu = gather_relay(wgu, *g_gu)
    r_dn = gather_relay(wdn, *g_dn)
    for c in c_s:
        c.wait_recv()
    srow = ssb[0]
    for b in range(1, NT):
        srow = srow + ssb[b]
    scol = jnp.sum(jnp.where(eye, jnp.broadcast_to(srow, (ROWS, 128)), 0.0), axis=1, keepdims=True)
    ffn = (middle * lax.rsqrt(scol * (1.0 / D) + EPS) * fgain[...]).astype(BF16)
    xall[z] = ffn
    c_x = []
    for d in range(1, NZ):
        i = nz()
        c_x.append(go(remote(xall.at[z], xall.at[z], zs.at[i], zr.at[i], at_z(d))))

    for c in c_r:
        c.wait_recv()
    rt = rout[...].astype(F32)
    shape3 = (NZ, ROWS, 128)
    lane3 = lax.broadcasted_iota(jnp.int32, shape3, 2)
    blk3 = lax.broadcasted_iota(jnp.int32, shape3, 0)
    sel = jnp.zeros(shape3, F32)
    hi = jnp.zeros(shape3, F32)
    lo = jnp.zeros(shape3, F32)
    for xx in range(NX):
        e = z * NX + xx
        r = jnp.sum(jnp.where(lane3 == e, rt, 0.0), axis=2, keepdims=True)
        wh = jnp.sum(jnp.where(lane3 == e + 32, rt, 0.0), axis=2, keepdims=True)
        wl = jnp.sum(jnp.where(lane3 == e + 64, rt, 0.0), axis=2, keepdims=True)
        place = blk3.astype(F32) * CAP + (r - 1.0) + float(xx * SLOTS)
        hit = (lane3.astype(F32) == place) & (r > 0.5)
        sel = sel + jnp.where(hit, 1.0, 0.0)
        hi = hi + jnp.where(hit, wh, 0.0)
        lo = lo + jnp.where(hit, wl, 0.0)
    ntok = NZ * ROWS
    selT = sel.reshape(ntok, 128).T.astype(BF16)
    hi2 = hi.reshape(ntok, 128).astype(BF16)
    lo2 = lo.reshape(ntok, 128).astype(BF16)

    for c in c_x:
        c.wait_recv()
    xs2 = xall[...].reshape(ntok, SL)
    picked = jnp.dot(selT, xs2, preferred_element_type=F32).astype(BF16)
    for xx in range(NX):
        esrc[xx] = picked[xx * SLOTS : (xx + 1) * SLOTS]
    c_e = []
    for d in range(1, NX):
        i = nx()
        xd = lax.rem(x + d, NX)
        c_e.append(go(remote(esrc.at[xd], eall.at[tp, x], xs.at[i], xr.at[i], at_x(d))))
    eall[tp, x] = esrc[x]

    for c in r_gu:
        c.wait_recv()
    for xx in range(NX):
        part = jnp.dot(xs2, wgu[xx], preferred_element_type=F32).astype(BF16)
        dsrc[:, :, xx * 256 : (xx + 1) * 256] = part.reshape(NZ, ROWS, 256)

    for c in c_e:
        c.wait_recv()
    c_ea = []
    for d in range(1, NT):
        i = nt()
        c_ea.append(go(remote(eall.at[tp], eall.at[tp], ts.at[i], tr.at[i], at_t(d))))
    c_d = []
    for d in range(1, NT):
        i = nt()
        td = lax.rem(tp + d, NT)
        c_d.append(go(remote(dsrc.at[td], ddst.at[tp], ts.at[i], tr.at[i], at_t(d))))
    ddst[tp] = dsrc[tp]

    for c in l_egu:
        c.wait()
    for c in c_ea:
        c.wait_recv()
    acc = jnp.zeros((NX * SLOTS, 256), F32)
    for t in range(NT):
        acc = acc + jnp.dot(
            eall[t].reshape(NX * SLOTS, SL), egu[t * SL : (t + 1) * SL, :], preferred_element_type=F32)
    ga, ua = acc[:, :128], acc[:, 128:]
    ehall[tp] = (ga / (1.0 + jnp.exp(-ga)) * ua).astype(BF16)
    c_eh = []
    for d in range(1, NT):
        i = nt()
        c_eh.append(go(remote(ehall.at[tp], ehall.at[tp], ts.at[i], tr.at[i], at_t(d))))

    for c in c_d:
        c.wait_recv()
    dsum = ddst[0].astype(F32)
    for b in range(1, NT):
        dsum = dsum + ddst[b].astype(F32)
    hid = []
    for xx in range(NX):
        g = dsum[:, xx * 256 : xx * 256 + 128]
        u = dsum[:, xx * 256 + 128 : xx * 256 + 256]
        hid.append((g / (1.0 + jnp.exp(-g)) * u).astype(BF16))
    hall[tp] = jnp.concatenate(hid, axis=1)
    c_h = []
    for d in range(1, NT):
        i = nt()
        c_h.append(go(remote(hall.at[tp], hall.at[tp], ts.at[i], tr.at[i], at_t(d))))

    l_ed.wait()
    for c in c_ed:
        c.wait_recv()
    for c in c_eh:
        c.wait_recv()
    eres = jnp.zeros((NX * SLOTS, SL), F32)
    for t in range(NT):
        eres = eres + jnp.dot(ehall[t], edn[t], preferred_element_type=F32)
    rsrc[...] = eres.astype(BF16).reshape(NX, SLOTS, SL)
    c_b = []
    for d in range(1, NX):
        i = nx()
        xd = lax.rem(x + d, NX)
        c_b.append(go(remote(rsrc.at[xd], rdst.at[x], xs.at[i], xr.at[i], at_x(d))))
    rdst[x] = rsrc[x]

    for c in r_dn:
        c.wait_recv()
    for c in c_h:
        c.wait_recv()
    down = jnp.dot(
        hall[...].reshape(ntok, SL), wdn[...].reshape(SL, SL), preferred_element_type=F32)
    down = down * (1.0 / (1.0 + jnp.exp(-mixv[...])))
    for c in c_b:
        c.wait_recv()
    back = rdst[...].reshape(NX * SLOTS, SL)
    down = down + jnp.dot(hi2[:, : NX * SLOTS], back, preferred_element_type=F32)
    down = down + jnp.dot(lo2[:, : NX * SLOTS], back, preferred_element_type=F32)
    fsrc[...] = down.astype(BF16).reshape(NZ, ROWS, SL)
    c_f = []
    for d in range(1, NZ):
        i = nz()
        zd = lax.rem(z + d, NZ)
        c_f.append(go(remote(fsrc.at[zd], fdst.at[z], zs.at[i], zr.at[i], at_z(d))))
    fdst[z] = fsrc[z]
    for c in c_f:
        c.wait_recv()
    total = middle
    for b in range(NZ):
        total = total + fdst[b].astype(F32)
    out_ref[...] = total.astype(BF16)

    for c in sent:
        c.wait_send()


def per_device(
    tokens, delta_state, attn_gain, query_weight, key_weight, value_weight, decay_weight, beta_weight, decay_rate,
    head_gain, output_weight, ffn_gain, expert_ids, group_prob, expert_logit, expert_gate, expert_up, expert_down,
    dense_gate, dense_up, dense_down, dense_mix,
):
    info = jnp.concatenate(
        (
            expert_ids.astype(F32),
            expert_logit,
            group_prob[:, None],
            jnp.zeros((ROWS, 123), F32),
        ),
        axis=1,
    )
    anyspec = pl.BlockSpec(memory_space=pl.ANY)
    in_specs = [anyspec] * 20
    in_specs[8] = pl.BlockSpec(memory_space=pltpu.SMEM)
    vm = pltpu.VMEM
    scratch = [
        vm((ROWS, D), BF16), vm((ROWS, SL), BF16), vm((1, D), F32), vm((3, NX, 128, 256), BF16), vm((2, 16, D), BF16),
        vm((1, HEAD), F32), vm((256, D), BF16), vm((1, SL), F32), vm((ROWS, 128), F32),
        vm((NX, SL, 256), BF16), vm((NX, 128, SL), BF16), vm((1, SL), F32), vm((D, 256), BF16), vm((NT, 128, SL), BF16),
        vm((ROWS, 2, HEAD, HEAD), F32),
        vm((NZ, ROWS, SL), BF16), vm((NZ, ROWS, SL), BF16),
        vm((3, NZ, ROWS, 256), BF16), vm((3, NZ, ROWS, 256), BF16), vm((NZ, ROWS, 128), BF16),
        vm((NT, ROWS, SL), BF16), vm((NT, ROWS, SL), BF16), vm((NT, 1, 128), F32), vm((NZ, ROWS, SL), BF16),
        vm((NT, ROWS, 1024), BF16), vm((NT, ROWS, 1024), BF16), vm((NT, ROWS, SL), BF16),
        vm((NX, SLOTS, SL), BF16), vm((NT, NX, SLOTS, SL), BF16), vm((NT, NX * SLOTS, 128), BF16),
        vm((NX, SLOTS, SL), BF16), vm((NX, SLOTS, SL), BF16), vm((NZ, ROWS, SL), BF16), vm((NZ, ROWS, SL), BF16),
        pltpu.SemaphoreType.DMA((24,)),
        pltpu.SemaphoreType.DMA((26,)), pltpu.SemaphoreType.DMA((26,)),
        pltpu.SemaphoreType.DMA((49,)), pltpu.SemaphoreType.DMA((49,)),
        pltpu.SemaphoreType.DMA((49,)), pltpu.SemaphoreType.DMA((49,)),
    ]
    mixed_out, new_state = pl.pallas_call(
        kernel,
        out_shape=(
            jax.ShapeDtypeStruct((ROWS, SL), BF16),
            jax.ShapeDtypeStruct((ROWS, 2, HEAD, HEAD), F32),
        ),
        in_specs=in_specs,
        out_specs=(pl.BlockSpec(memory_space=pltpu.VMEM), pl.BlockSpec(memory_space=pltpu.VMEM)),
        scratch_shapes=scratch,
        compiler_params=pltpu.CompilerParams(
            collective_id=0, has_side_effects=True, vmem_limit_bytes=48 * 1024 * 1024),
        name="layer",
    )(
        tokens, delta_state, attn_gain.reshape(1, D), query_weight, key_weight, value_weight, decay_weight.T,
        beta_weight.T, decay_rate, head_gain.reshape(1, HEAD), output_weight, ffn_gain.reshape(1, D), info,
        expert_gate.reshape(D, 128), expert_up.reshape(D, 128), expert_down.reshape(128, D), dense_gate, dense_up,
        dense_down, dense_mix.reshape(1, SL),
    )
    return mixed_out, new_state


def solution(mesh):
    return jax.shard_map(
        per_device,
        mesh=mesh,
        in_specs=(
            P("ep", None),
            P("ep", "tp", None, None),
            P(),
            P("ep", "tp"),
            P("ep", "tp"),
            P("ep", "tp"),
            P(),
            P(),
            P("tp"),
            P(),
            P("tp", None),
            P(),
            P("ep", None),
            P("ep"),
            P("ep", None),
            P("ep", None, "tp"),
            P("ep", None, "tp"),
            P("ep", "tp", None),
            P("tp", "ep"),
            P("tp", "ep"),
            P("ep", "tp"),
            P("tp"),
        ),
        out_specs=(P("ep", "tp"), P("ep", "tp", None, None)),
        check_vma=False,
    )
```

```python
import jax
import jax.numpy as jnp
from jax import lax
from jax.experimental import pallas as pl
from jax.experimental.pallas import tpu as pltpu
from jax.sharding import PartitionSpec as P

EPS = 1e-06
MESH = pl.DeviceIdType.MESH
F32 = jnp.float32
BF16 = jnp.bfloat16

NX, NZ, NY, NT = 4, 8, 4, 8
ROWS = 24
D = 4096
SL = 512
HEAD = 128
CAP = 3
SLOTS = NZ * CAP
N_SEND, N_RECV = 23, 52
X_ORDER = (2, 1, 3)
Z_ORDER = (4, 3, 5, 2, 6, 1, 7)
Y_ORDER = (2, 1, 3)
E_ORDER = tuple(
    (dx, dy) for far in (4, 3, 2, 1) for dx in range(NX) for dy in range(NY)
    if min(dx, NX - dx) + min(dy, NY - dy) == far)
T_ORDER = ((2, 0), (2, 1), (1, 0), (1, 1), (3, 0), (3, 1), (0, 1))


def kernel(
    tok_h, state_h, again_h, wq_h, wk_h, wv_h, dT_h, bT_h, rate_h, hgain_h, wo_h, fgain_h, ids_h,
    lgt_h, prob_h,
    eg_h, eu_h, ed_h, dg_h, du_h, dd_h, mix_h,
    out_ref, state_o,
    tok, tokf, again, wqkv, db, rate, hgain, wo, fgain, idv, lgv, prv, wgu, wdn, mixv, egu, edn, state,
    spread, act, psrc, pdst, rout, asrc, adst, ssb, rsb, xall, dsrc, dmate, dpair, ddst, qsrc, qdst, hall, esrc, eall, ehall, rsrc, rdst, fsrc, fdst,
    lsem, ssem, rsem,
):
    ep = lax.axis_index("ep")
    tp = lax.axis_index("tp")
    z = ep // NX
    x = lax.rem(ep, NX)

    def at_x(d):
        return {"ep": z * NX + lax.rem(x + d, NX), "tp": tp}

    def at_z(d):
        return {"ep": lax.rem(z + d, NZ) * NX + x, "tp": tp}

    y = tp // 2
    core = lax.rem(tp, 2)

    def t_index(d):
        return lax.rem(y + d[0], NY) * 2 + lax.rem(core + d[1], 2)

    def at_t(d):
        return {"ep": ep, "tp": t_index(d)}

    other = 1 - core
    mate = {"ep": ep, "tp": y * 2 + other}

    def y_index(d):
        return lax.rem(y + d, NY) * 2 + core

    def at_y(d):
        return {"ep": ep, "tp": y_index(d)}

    def remote(src, dst, ss, rs, dev):
        return pltpu.make_async_remote_copy(
            src_ref=src, dst_ref=dst, send_sem=ss, recv_sem=rs, device_id=dev, device_id_type=MESH
        )

    count = {"send": 0, "recv": 0}
    last = []

    def new(kind):
        count[kind] += 1
        return count[kind] - 1

    def send(src, dst, si, ri, dev):
        copy = remote(src, dst, ssem.at[si], rsem.at[ri], dev)
        copy.start()
        return copy

    def leaves(whole, si):
        last.append(remote(whole, whole, ssem.at[si], rsem.at[0], mate))

    def exchange(order, at, src, dst, whole):
        si, ri = new("send"), new("recv")
        for d in order:
            send(src(d), dst, si, ri, at(d))
        leaves(whole, si)
        return remote(whole, whole, ssem.at[si], rsem.at[ri], mate)

    local = []

    def load(src, dst):
        c = pltpu.make_async_copy(src, dst, lsem.at[len(local)])
        c.start()
        local.append(c)
        return c

    bar = pltpu.get_barrier_semaphore()
    for d in X_ORDER:
        pl.semaphore_signal(bar, inc=1, device_id=at_x(d), device_id_type=MESH)
    for d in Z_ORDER:
        pl.semaphore_signal(bar, inc=1, device_id=at_z(d), device_id_type=MESH)
    for d in T_ORDER:
        pl.semaphore_signal(bar, inc=1, device_id=at_t(d), device_id_type=MESH)

    l_tok = load(tok_h, tok)
    l_again = load(again_h, again)
    l_w = [load(w, wqkv.at[m, x]) for m, w in enumerate((wk_h, wq_h, wv_h))]

    pl.semaphore_wait(bar, NX + NZ + NT - 3)

    left = lax.rem(x + NX - 1, NX)
    right = lax.rem(x + 1, NX)

    def gather_start(buf, si):
        return (
            send(buf.at[x], buf.at[x], si, new("recv"), at_x(1)),
            send(buf.at[x], buf.at[x], si, new("recv"), at_x(NX - 1)),
        )

    def gather_relay(buf, si, c0, c1):
        h = buf.shape[1] // 2
        low, high = buf.at[left, pl.ds(0, h)], buf.at[right, pl.ds(h, h)]
        c0.wait_recv()
        r0 = send(low, low, si, new("recv"), at_x(1))
        c1.wait_recv()
        r1 = send(high, high, si, new("recv"), at_x(NX - 1))
        return r0, r1

    for c in l_w:
        c.wait()
    s_w = new("send")
    leaves(wqkv.at[:, pl.ds(0, 3)], s_w)
    g_w = [gather_start(wqkv.at[m], s_w) for m in range(2)]

    l_tok.wait()
    l_again.wait()
    t32 = tok[...].astype(F32)
    ms = jnp.sum(t32 * t32, axis=1, keepdims=True) * (1.0 / D)
    normed = (t32 * lax.rsqrt(ms + EPS) * again[...]).astype(BF16)
    for b in range(NZ):
        for h in range(2):
            spread[h, b] = normed[:, b * SL + h * 256 : b * SL + (h + 1) * 256]

    c_spread = exchange(
        Z_ORDER, at_z, lambda d: spread.at[core, lax.rem(z + d, NZ)], act.at[core, z], act.at[core, pl.ds(0, NZ - 1)])
    act[core, z] = spread[core, z]

    c_ed = exchange(
        T_ORDER, at_t, lambda d: ed_h.at[:, pl.ds(pl.multiple_of(t_index(d) * SL, SL), SL)], edn.at[tp],
        edn.at[pl.ds(0, NT - 1)])

    l_db = [load(dT_h, db.at[0]), load(bT_h, db.at[1]), load(rate_h, rate)]
    l_info = [load(ids_h, idv), load(lgt_h, lgv), load(prob_h, prv)]
    l_gu = [load(dg_h, wgu.at[x, :, pl.ds(0, 128)]), load(du_h, wgu.at[x, :, pl.ds(128, 128)])]
    l_dn = load(dd_h, wdn.at[x])
    l_state = load(state_h, state)
    l_wo = load(wo_h, wo)
    l_small = [
        load(hgain_h, hgain),
        load(fgain_h.at[:, pl.ds(pl.multiple_of(tp * SL, SL), SL)], fgain),
        load(mix_h, mixv),
        load(tok_h.at[:, pl.ds(pl.multiple_of(tp * SL, SL), SL)], tokf),
    ]
    l_ed = load(ed_h.at[:, pl.ds(pl.multiple_of(tp * SL, SL), SL)], edn.at[tp])
    l_egu = [load(eg_h, egu.at[:, pl.ds(0, 128)]), load(eu_h, egu.at[:, pl.ds(128, 128)])]

    for c in l_db:
        c.wait()
    dims = (((1,), (1,)), ((), ()))
    dpre = lax.dot_general(normed, db[0], dims, preferred_element_type=F32)
    bpre = lax.dot_general(normed, db[1], dims, preferred_element_type=F32)
    lane16 = lax.broadcasted_iota(jnp.int32, dpre.shape, 1)
    decay, beta = [], []
    for h in range(2):
        pick = lane16 == tp * 2 + h
        dp = jnp.sum(jnp.where(pick, dpre, 0.0), axis=1, keepdims=True)
        bp = jnp.sum(jnp.where(pick, bpre, 0.0), axis=1, keepdims=True)
        soft = jnp.maximum(dp, 0.0) + jnp.log(1.0 + jnp.exp(-jnp.abs(dp)))
        decay.append(jnp.exp(-rate[:, h : h + 1] * soft))
        beta.append(1.0 / (1.0 + jnp.exp(-bp)))

    for c in l_info:
        c.wait()
    ex = jnp.exp(lgv[...])
    wrow = prv[...] * ex / (ex[0:1] + ex[1:2])
    idf = idv[...].astype(F32)
    square = (ROWS, ROWS)
    eye24 = lax.broadcasted_iota(jnp.int32, square, 0) == lax.broadcasted_iota(jnp.int32, square, 1)

    def column(row):
        return jnp.sum(jnp.where(eye24, jnp.broadcast_to(row, square), 0.0), axis=1, keepdims=True)

    id0, id1 = column(idf[0:1]), column(idf[1:2])
    w0, w1 = column(wrow[0:1]), column(wrow[1:2])
    lanef = lax.broadcasted_iota(jnp.int32, (ROWS, 128), 1).astype(F32)
    rowi = lax.broadcasted_iota(jnp.int32, (ROWS, 128), 0)
    oh = jnp.where((lanef == id0) | (lanef == id1), 1.0, 0.0)
    rank = jnp.zeros((ROWS, 128), F32)
    for i in range(ROWS - 1):
        rank = rank + jnp.where(rowi > i, oh[i : i + 1, :], 0.0)
    table = (rank + 1.0) * oh
    for idk, wk in ((id0, w0), (id1, w1)):
        whi = wk.astype(BF16).astype(F32)
        table = table + jnp.where(lanef == idk + 32.0, whi, 0.0)
        table = table + jnp.where(lanef == idk + 64.0, wk - whi, 0.0)
    rout[z] = table.astype(BF16)

    r_w = [gather_relay(wqkv.at[0], s_w, *g_w[0])]
    g_v = gather_start(wqkv.at[2], s_w)
    r_w.append(gather_relay(wqkv.at[1], s_w, *g_w[1]))
    c_spread.wait_recv()
    i = new("send")
    c_share = send(act.at[core], act.at[core], i, new("recv"), mate)
    leaves(act.at[core], i)
    for c in r_w[0]:
        c.wait_recv()
    ntok = NZ * ROWS

    def half(m, h):
        return jnp.dot(
            act[h].reshape(ntok, 256), wqkv[m, pl.ds(h * 2, 2)].reshape(256, 256), preferred_element_type=F32)

    c_p = []
    for m in range(3):
        if m:
            for c in r_w[m]:
                c.wait_recv()
        part = half(m, core)
        if m == 0:
            c_share.wait_recv()
        part = part + half(m, other)
        psrc[m] = part.astype(BF16).reshape(NZ, ROWS, 2 * HEAD)
        c_p.append(exchange(
            Z_ORDER, at_z, lambda d: psrc.at[m, lax.rem(z + d, NZ)], pdst.at[m, z], pdst.at[m, pl.ds(0, NZ - 1)]))
        pdst[m, z] = psrc[m, z]
        if m == 0:
            r_w.append(gather_relay(wqkv.at[2], s_w, *g_v))
    for c in l_gu:
        c.wait()
    l_dn.wait()
    s_gu, s_dn = new("send"), new("send")
    g_gu = gather_start(wgu, s_gu)
    g_dn = gather_start(wdn, s_dn)
    leaves(wgu.at[pl.ds(0, 3)], s_gu)
    leaves(wdn.at[pl.ds(0, 3)], s_dn)

    c_r = exchange(Z_ORDER, at_z, lambda d: rout.at[z], rout.at[z], rout.at[pl.ds(0, NZ - 1)])

    def arrived(m):
        c_p[m].wait_recv()
        total = pdst[m, 0].astype(F32)
        for b in range(1, NZ):
            total = total + pdst[m, b].astype(F32)
        return total.astype(BF16).astype(F32)

    def unit(rows):
        return rows * lax.rsqrt(jnp.sum(rows * rows, axis=1, keepdims=True) + EPS)

    def read_state(h, cols):
        return jnp.concatenate(
            [jnp.sum(state[b, h] * cols[:, b : b + 1], axis=0, keepdims=True) for b in range(ROWS)], axis=0)

    l_state.wait()
    rows_k = arrived(0)
    ku = [unit(rows_k[:, h * HEAD : (h + 1) * HEAD]) for h in range(2)]
    kT = [u.T for u in ku]
    rec = [read_state(h, kT[h]) for h in range(2)]
    rows_q = arrived(1)
    qu = [unit(rows_q[:, h * HEAD : (h + 1) * HEAD]) * HEAD ** (-0.5) for h in range(2)]
    red = [read_state(h, qu[h].T) for h in range(2)]
    for c in l_small:
        c.wait()
    l_wo.wait()
    rows_v = arrived(2)
    heads, corrs = [], []
    for h in range(2):
        kq = jnp.sum(ku[h] * qu[h], axis=1, keepdims=True)
        corr = beta[h] * (rows_v[:, h * HEAD : (h + 1) * HEAD] - decay[h] * rec[h])
        ro = decay[h] * red[h] + kq * corr
        ro = ro * lax.rsqrt(jnp.mean(ro * ro, axis=1, keepdims=True) + EPS) * hgain[...]
        heads.append(ro.astype(BF16))
        corrs.append(corr)

    hcat = jnp.concatenate(heads, axis=1)
    si, ri = new("send"), new("recv")
    for d in T_ORDER + ((0, 0),):
        td = t_index(d)
        cols = wo[:, pl.ds(pl.multiple_of(td * SL, SL), SL)]
        asrc[td] = jnp.dot(hcat, cols, preferred_element_type=F32).astype(BF16)
        if d != (0, 0):
            send(asrc.at[td], adst.at[tp], si, ri, at_t(d))
    whole = adst.at[pl.ds(0, NT - 1)]
    leaves(whole, si)
    c_a = remote(whole, whole, ssem.at[si], rsem.at[ri], mate)
    adst[tp] = asrc[tp]

    for h in range(2):
        for b in range(ROWS):
            state[b, h] = state[b, h] * decay[h][b : b + 1, :] + kT[h][:, b : b + 1] * corrs[h][b : b + 1, :]
    w_state = pltpu.make_async_copy(state, state_o, lsem.at[len(local)])
    w_state.start()

    c_a.wait_recv()
    asum = adst[0].astype(F32)
    for b in range(1, NT):
        asum = asum + adst[b].astype(F32)
    middle = tokf[...].astype(F32) + asum
    ss = jnp.sum(middle * middle, axis=1, keepdims=True)
    eye = lax.broadcasted_iota(jnp.int32, (ROWS, 128), 0) == lax.broadcasted_iota(jnp.int32, (ROWS, 128), 1)
    ssb[tp] = jnp.sum(jnp.where(eye, ss, 0.0), axis=0, keepdims=True)
    c_s = exchange(T_ORDER, at_t, lambda d: ssb.at[tp], ssb.at[tp], ssb.at[pl.ds(0, NT - 1)])
    xall[z] = (middle * fgain[...]).astype(BF16)
    c_x = exchange(Z_ORDER, at_z, lambda d: xall.at[z], xall.at[z], xall.at[pl.ds(0, NZ - 1)])
    r_gu = gather_relay(wgu, s_gu, *g_gu)
    r_dn = gather_relay(wdn, s_dn, *g_dn)
    c_s.wait_recv()
    srow = ssb[0]
    for b in range(1, NT):
        srow = srow + ssb[b]
    rsb[z] = lax.rsqrt(srow * (1.0 / D) + EPS)
    c_q = exchange(Z_ORDER, at_z, lambda d: rsb.at[z], rsb.at[z], rsb.at[pl.ds(0, NZ - 1)])

    c_r.wait_recv()
    rt = rout[...].astype(F32)
    shape3 = (NZ, ROWS, 128)
    lane3 = lax.broadcasted_iota(jnp.int32, shape3, 2)
    blk3 = lax.broadcasted_iota(jnp.int32, shape3, 0)
    sel = jnp.zeros(shape3, F32)
    hi = jnp.zeros(shape3, F32)
    lo = jnp.zeros(shape3, F32)
    for xx in range(NX):
        e = z * NX + xx
        r = jnp.sum(jnp.where(lane3 == e, rt, 0.0), axis=2, keepdims=True)
        wh = jnp.sum(jnp.where(lane3 == e + 32, rt, 0.0), axis=2, keepdims=True)
        wl = jnp.sum(jnp.where(lane3 == e + 64, rt, 0.0), axis=2, keepdims=True)
        place = blk3.astype(F32) * CAP + (r - 1.0) + float(xx * SLOTS)
        hit = (lane3.astype(F32) == place) & (r > 0.5)
        sel = sel + jnp.where(hit, 1.0, 0.0)
        hi = hi + jnp.where(hit, wh, 0.0)
        lo = lo + jnp.where(hit, wl, 0.0)
    selT = sel.reshape(ntok, 128).T.astype(BF16)
    hi2 = hi.reshape(ntok, 128).astype(BF16)
    lo2 = lo.reshape(ntok, 128).astype(BF16)

    c_x.wait_recv()
    xs2 = xall[...].reshape(ntok, SL)
    picked = jnp.dot(selT, xs2, preferred_element_type=F32).astype(BF16)
    for xx in range(NX):
        esrc[xx] = picked[xx * SLOTS : (xx + 1) * SLOTS]
    si = new("send")
    r_e = {d: new("recv") for d in (0,) + Y_ORDER}
    for dx, dy in E_ORDER:
        xd = lax.rem(x + dx, NX)
        dev = {"ep": z * NX + xd, "tp": y_index(dy)}
        send(esrc.at[xd], eall.at[tp, x], si, r_e[dy], dev)
    leaves(eall.at[pl.ds(0, 3)], si)
    leaves_e = eall.at[0, pl.ds(0, NX - 1)]
    leaves(leaves_e, si)
    eall[tp, x] = esrc[x]

    for c in r_gu:
        c.wait_recv()
    for xx in range(NX):
        part = jnp.dot(xs2, wgu[xx], preferred_element_type=F32).astype(BF16).reshape(NZ, ROWS, 256)
        for b in range(NZ):
            dsrc[b % 2, b // 2, :, xx * 256 : (xx + 1) * 256] = part[b]
    c_q.wait_recv()
    eye3 = lax.broadcasted_iota(jnp.int32, shape3, 1) == lane3
    rcol = jnp.sum(jnp.where(eye3, jnp.broadcast_to(rsb[...], shape3), 0.0), axis=2, keepdims=True)
    rhi = rcol.astype(BF16).astype(F32)
    pair = jnp.where(lane3 < 64, rhi, rcol - rhi).astype(BF16).reshape(ntok, 128)
    rslot = jnp.dot(selT, pair, preferred_element_type=F32)
    rslot = jnp.broadcast_to(rslot[:, 0:1] + rslot[:, 127:128], (128, 128))
    for xx in range(NX):
        qsrc[xx] = rslot[xx * SLOTS : (xx + 1) * SLOTS]
    c_sc = exchange(
        X_ORDER, at_x, lambda d: qsrc.at[lax.rem(x + d, NX)], qdst.at[x], qdst.at[pl.ds(0, NX - 1)])
    qdst[x] = qsrc[x]
    i = new("send")
    c_dm = send(dsrc.at[other], dmate, i, new("recv"), mate)
    leaves(dmate, i)
    for c in l_egu:
        c.wait()
    c_dm.wait_recv()
    for b in range(NY):
        dpair[b] = (dsrc[core, b].astype(F32) + dmate[b].astype(F32)).astype(BF16)
    c_d = exchange(
        Y_ORDER, at_y, lambda d: dpair.at[lax.rem(y + d, NY)], ddst.at[y], ddst.at[pl.ds(0, NY - 1)])
    ddst[y] = dpair[y]

    def hidden_part(t):
        rows = egu[pl.ds(pl.multiple_of(t * SL, SL), SL), :]
        return jnp.dot(eall[t].reshape(NX * SLOTS, SL), rows, preferred_element_type=F32)

    s_m = new("send")
    acc = jnp.zeros((NX * SLOTS, 256), F32)
    c_m = []
    for dy in (0, 1, 3, 2):
        t = y_index(NY - dy)
        got = eall.at[t] if dy else leaves_e
        remote(got, got, ssem.at[si], rsem.at[r_e[dy]], mate).wait_recv()
        c_m.append(send(eall.at[t], eall.at[t], s_m, new("recv"), mate))
        acc = acc + hidden_part(t)
    leaves(eall.at[pl.ds(0, NY)], s_m)
    for c, dy in zip(c_m, (0, 1, 3, 2)):
        c.wait_recv()
        acc = acc + hidden_part(lax.rem(y + NY - dy, NY) * 2 + other)

    def tp_gather(buf):
        si, rm = new("send"), new("recv")
        out = [send(buf.at[tp], buf.at[tp], si, new("recv"), at_y(d)) for d in Y_ORDER]
        send(buf.at[tp], buf.at[tp], si, rm, mate)
        return si, rm, out

    def tp_gathered(buf, si, rm, out):
        for c, d in zip(out, Y_ORDER):
            c.wait_recv()
            t = y_index(NY - d)
            send(buf.at[t], buf.at[t], si, rm, mate)
        leaves(buf.at[pl.ds(0, NT - 1)], si)
        got = buf.at[pl.ds(0, NY)]
        remote(got, got, ssem.at[si], rsem.at[rm], mate).wait_recv()

    c_sc.wait_recv()
    scale = qdst[...].reshape(NX * SLOTS, 128)
    ga, ua = acc[:, :128] * scale, acc[:, 128:] * scale
    ehall[tp] = (ga / (1.0 + jnp.exp(-ga)) * ua).astype(BF16)
    c_eh = tp_gather(ehall)

    c_d.wait_recv()
    dsum = ddst[0].astype(F32)
    for b in range(1, NY):
        dsum = dsum + ddst[b].astype(F32)
    dsum = dsum * jnp.sum(jnp.where(eye, jnp.broadcast_to(rsb[tp], (ROWS, 128)), 0.0), axis=1, keepdims=True)
    hid = []
    for xx in range(NX):
        g = dsum[:, xx * 256 : xx * 256 + 128]
        u = dsum[:, xx * 256 + 128 : xx * 256 + 256]
        hid.append((g / (1.0 + jnp.exp(-g)) * u).astype(BF16))
    hall[tp] = jnp.concatenate(hid, axis=1)
    c_h = tp_gather(hall)

    l_ed.wait()
    c_ed.wait_recv()
    tp_gathered(ehall, *c_eh)
    eres = jnp.zeros((NX * SLOTS, SL), F32)
    for t in range(NT):
        eres = eres + jnp.dot(ehall[t], edn[t], preferred_element_type=F32)
    rsrc[...] = eres.astype(BF16).reshape(NX, SLOTS, SL)
    c_b = exchange(
        X_ORDER, at_x, lambda d: rsrc.at[lax.rem(x + d, NX)], rdst.at[x], rdst.at[pl.ds(0, NX - 1)])
    rdst[x] = rsrc[x]

    for c in r_dn:
        c.wait_recv()
    tp_gathered(hall, *c_h)
    down = jnp.dot(
        hall[...].reshape(ntok, SL), wdn[...].reshape(SL, SL), preferred_element_type=F32)
    down = down * (1.0 / (1.0 + jnp.exp(-mixv[...])))
    c_b.wait_recv()
    back = rdst[...].reshape(NX * SLOTS, SL)
    down = down + jnp.dot(hi2[:, : NX * SLOTS], back, preferred_element_type=F32)
    down = down + jnp.dot(lo2[:, : NX * SLOTS], back, preferred_element_type=F32)
    fsrc[...] = down.astype(BF16).reshape(NZ, ROWS, SL)
    c_f = exchange(
        Z_ORDER, at_z, lambda d: fsrc.at[lax.rem(z + d, NZ)], fdst.at[z], fdst.at[pl.ds(0, NZ - 1)])
    fdst[z] = fsrc[z]
    c_f.wait_recv()
    total = middle
    for b in range(NZ):
        total = total + fdst[b].astype(F32)
    out_ref[...] = total.astype(BF16)

    for c in last:
        c.wait_send()
    w_state.wait()
    assert count == {"send": N_SEND, "recv": N_RECV}, count


def per_device(
    tokens, delta_state, attn_gain, query_weight, key_weight, value_weight, decay_weight, beta_weight, decay_rate,
    head_gain, output_weight, ffn_gain, expert_ids, group_prob, expert_logit, expert_gate, expert_up, expert_down,
    dense_gate, dense_up, dense_down, dense_mix,
):
    hbm = pl.BlockSpec(memory_space=pltpu.HBM)
    in_specs = [hbm] * 22
    vm = pltpu.VMEM
    scratch = [
        vm((ROWS, D), BF16), vm((ROWS, SL), BF16), vm((1, D), F32), vm((3, NX, 128, 256), BF16), vm((2, 16, D), BF16),
        vm((1, 2), F32),        vm((1, HEAD), F32), vm((256, D), BF16), vm((1, SL), F32), vm((2, ROWS), jnp.int32),
        vm((2, ROWS), F32), vm((1, ROWS), F32), vm((NX, SL, 256), BF16), vm((NX, 128, SL), BF16), vm((1, SL), F32), vm((D, 256), BF16), vm((NT, 128, SL), BF16),
        vm((ROWS, 2, HEAD, HEAD), F32),
        vm((2, NZ, ROWS, 256), BF16), vm((2, NZ, ROWS, 256), BF16),
        vm((3, NZ, ROWS, 256), BF16), vm((3, NZ, ROWS, 256), BF16), vm((NZ, ROWS, 128), BF16),
        vm((NT, ROWS, SL), BF16), vm((NT, ROWS, SL), BF16), vm((NT, 1, 128), F32), vm((NZ, 1, 128), F32),
        vm((NZ, ROWS, SL), BF16),
        vm((2, NY, ROWS, 1024), BF16), vm((NY, ROWS, 1024), BF16), vm((NY, ROWS, 1024), BF16),
        vm((NY, ROWS, 1024), BF16), vm((NX, SLOTS, 128), F32), vm((NX, SLOTS, 128), F32), vm((NT, ROWS, SL), BF16),
        vm((NX, SLOTS, SL), BF16), vm((NT, NX, SLOTS, SL), BF16), vm((NT, NX * SLOTS, 128), BF16),
        vm((NX, SLOTS, SL), BF16), vm((NX, SLOTS, SL), BF16), vm((NZ, ROWS, SL), BF16), vm((NZ, ROWS, SL), BF16),
        pltpu.SemaphoreType.DMA((32,)),
        pltpu.SemaphoreType.DMA((N_SEND,)), pltpu.SemaphoreType.DMA((N_RECV,)),
    ]
    operands = (
        tokens, delta_state, attn_gain.reshape(1, D), query_weight, key_weight, value_weight, decay_weight.T,
        beta_weight.T, decay_rate.reshape(1, 2), head_gain.reshape(1, HEAD), output_weight, ffn_gain.reshape(1, D), expert_ids.T,
        expert_logit.T, group_prob.reshape(1, ROWS), expert_gate.reshape(D, 128), expert_up.reshape(D, 128),
        expert_down.reshape(128, D), dense_gate, dense_up, dense_down, dense_mix.reshape(1, SL),
    )
    operands = [pltpu.with_memory_space_constraint(o, pltpu.HBM) for o in operands]
    mixed_out, new_state = pl.pallas_call(
        kernel,
        out_shape=(
            jax.ShapeDtypeStruct((ROWS, SL), BF16),
            jax.ShapeDtypeStruct((ROWS, 2, HEAD, HEAD), F32),
        ),
        in_specs=in_specs,
        out_specs=(pl.BlockSpec(memory_space=pltpu.VMEM), pl.BlockSpec(memory_space=pl.ANY)),
        scratch_shapes=scratch,
        compiler_params=pltpu.CompilerParams(
            collective_id=0, has_side_effects=True, vmem_limit_bytes=24 * 1024 * 1024),
        name="layer",
    )(*operands)
    return mixed_out, new_state


def solution(mesh):
    return jax.shard_map(
        per_device,
        mesh=mesh,
        in_specs=(
            P("ep", None),
            P("ep", "tp", None, None),
            P(),
            P("ep", "tp"),
            P("ep", "tp"),
            P("ep", "tp"),
            P(),
            P(),
            P("tp"),
            P(),
            P("tp", None),
            P(),
            P("ep", None),
            P("ep"),
            P("ep", None),
            P("ep", None, "tp"),
            P("ep", None, "tp"),
            P("ep", "tp", None),
            P("tp", "ep"),
            P("tp", "ep"),
            P("ep", "tp"),
            P("tp"),
        ),
        out_specs=(P("ep", "tp"), P("ep", "tp", None, None)),
        check_vma=False,
    )
```

```python
import jax
import jax.numpy as jnp
from jax import lax
from jax.experimental import pallas as pl
from jax.experimental.pallas import tpu as pltpu
from jax.sharding import PartitionSpec as P

EPS = 1e-06
MESH = pl.DeviceIdType.MESH
F32 = jnp.float32
BF16 = jnp.bfloat16

NX, NZ, NY, NT = 4, 8, 4, 8
ROWS = 24
D = 4096
SL = 512
HEAD = 128
CAP = 3
SLOTS = NZ * CAP
N_SEND, N_RECV = 24, 49
X_ORDER = (2, 1, 3)
Z_ORDER = (4, 3, 5, 2, 6, 1, 7)
Y_ORDER = (2, 1, 3)
E_ORDER = tuple(
    (dx, dy) for far in (4, 3, 2, 1) for dy in Y_ORDER + (0,) for dx in X_ORDER + (0,)
    if min(dx, NX - dx) + min(dy, NY - dy) == far)
T_ORDER = ((2, 0), (2, 1), (1, 0), (1, 1), (3, 0), (3, 1), (0, 1))


def kernel(
    tok_h, state_h, again_h, wq_h, wk_h, wv_h, dT_h, bT_h, rate_h, hgain_h, wo_h, fgain_h, ids_h,
    lgt_h, prob_h,
    eg_h, eu_h, ed_h, dg_h, du_h, dd_h, mix_h,
    out_ref, state_o,
    tok, tokf, again, wqkv, db, rate, hgain, wo, fgain, idv, lgv, prv, wgu, wdn, mixv, egu, edn, state,
    spread, act, psrc, pdst, rout, asrc, adst, ssb, rsb, xall, dsrc, dmate, dpair, ddst, qsrc, qdst, hall, esrc, eall, ehall, rsrc, rdst, fsrc, fdst,
    lsem, ssem, rsem,
):
    ep = lax.axis_index("ep")
    tp = lax.axis_index("tp")
    z = ep // NX
    x = lax.rem(ep, NX)

    def at_x(d):
        return {"ep": z * NX + lax.rem(x + d, NX), "tp": tp}

    def at_z(d):
        return {"ep": lax.rem(z + d, NZ) * NX + x, "tp": tp}

    y = tp // 2
    core = lax.rem(tp, 2)

    def t_index(d):
        return lax.rem(y + d[0], NY) * 2 + lax.rem(core + d[1], 2)

    def at_t(d):
        return {"ep": ep, "tp": t_index(d)}

    other = 1 - core
    mate = {"ep": ep, "tp": y * 2 + other}

    def y_index(d):
        return lax.rem(y + d, NY) * 2 + core

    def at_y(d):
        return {"ep": ep, "tp": y_index(d)}

    def remote(src, dst, ss, rs, dev):
        return pltpu.make_async_remote_copy(
            src_ref=src, dst_ref=dst, send_sem=ss, recv_sem=rs, device_id=dev, device_id_type=MESH
        )

    count = {"send": 0, "recv": 0}
    last = []

    def new(kind):
        count[kind] += 1
        return count[kind] - 1

    def send(src, dst, si, ri, dev):
        copy = remote(src, dst, ssem.at[si], rsem.at[ri], dev)
        copy.start()
        return copy

    def leaves(whole, si):
        last.append(remote(whole, whole, ssem.at[si], rsem.at[0], mate))

    def exchange(order, at, src, dst, whole):
        si, ri = new("send"), new("recv")
        for d in order:
            send(src(d), dst, si, ri, at(d))
        leaves(whole, si)
        return remote(whole, whole, ssem.at[si], rsem.at[ri], mate)

    local = []

    def load(src, dst):
        c = pltpu.make_async_copy(src, dst, lsem.at[len(local)])
        c.start()
        local.append(c)
        return c

    bar = pltpu.get_barrier_semaphore()
    for d in X_ORDER:
        pl.semaphore_signal(bar, inc=1, device_id=at_x(d), device_id_type=MESH)
    for d in Z_ORDER:
        pl.semaphore_signal(bar, inc=1, device_id=at_z(d), device_id_type=MESH)
    for d in T_ORDER:
        pl.semaphore_signal(bar, inc=1, device_id=at_t(d), device_id_type=MESH)

    l_tok = load(tok_h, tok)
    l_again = load(again_h, again)
    l_w = [load(w, wqkv.at[m, x]) for m, w in enumerate((wk_h, wq_h, wv_h))]

    pl.semaphore_wait(bar, NX + NZ + NT - 3)

    left = lax.rem(x + NX - 1, NX)
    right = lax.rem(x + 1, NX)

    def gather_start(buf, si):
        return (
            send(buf.at[x], buf.at[x], si, new("recv"), at_x(1)),
            send(buf.at[x], buf.at[x], si, new("recv"), at_x(NX - 1)),
        )

    def gather_relay(buf, si, c0, c1):
        h = buf.shape[1] // 2
        low, high = buf.at[left, pl.ds(0, h)], buf.at[right, pl.ds(h, h)]
        c0.wait_recv()
        r0 = send(low, low, si, new("recv"), at_x(1))
        c1.wait_recv()
        r1 = send(high, high, si, new("recv"), at_x(NX - 1))
        return r0, r1

    for c in l_w:
        c.wait()
    s_w = new("send")
    leaves(wqkv.at[pl.ds(0, 2), pl.ds(0, 3)], s_w)
    g_w = [gather_start(wqkv.at[m], s_w) for m in range(2)]

    l_tok.wait()
    l_again.wait()
    t32 = tok[...].astype(F32)
    ms = jnp.sum(t32 * t32, axis=1, keepdims=True) * (1.0 / D)
    normed = (t32 * lax.rsqrt(ms + EPS) * again[...]).astype(BF16)
    for b in range(NZ):
        for h in range(2):
            spread[h, b] = normed[:, b * SL + h * 256 : b * SL + (h + 1) * 256]

    c_spread = exchange(
        Z_ORDER, at_z, lambda d: spread.at[core, lax.rem(z + d, NZ)], act.at[core, z], act.at[core, pl.ds(0, NZ - 1)])
    act[core, z] = spread[core, z]

    c_ed = exchange(
        T_ORDER, at_t, lambda d: ed_h.at[:, pl.ds(pl.multiple_of(t_index(d) * SL, SL), SL)], edn.at[tp],
        edn.at[pl.ds(0, NT - 1)])

    l_db = [load(dT_h, db.at[0]), load(bT_h, db.at[1]), load(rate_h, rate)]
    l_info = [load(ids_h, idv), load(lgt_h, lgv), load(prob_h, prv)]
    l_gu = [load(dg_h, wgu.at[x, :, pl.ds(0, 128)]), load(du_h, wgu.at[x, :, pl.ds(128, 128)])]
    l_dn = load(dd_h, wdn.at[x])
    l_state = load(state_h, state)
    l_wo = load(wo_h, wo)
    l_small = [
        load(hgain_h, hgain),
        load(fgain_h.at[:, pl.ds(pl.multiple_of(tp * SL, SL), SL)], fgain),
        load(mix_h, mixv),
        load(tok_h.at[:, pl.ds(pl.multiple_of(tp * SL, SL), SL)], tokf),
    ]
    l_ed = load(ed_h.at[:, pl.ds(pl.multiple_of(tp * SL, SL), SL)], edn.at[tp])
    l_egu = [load(eg_h, egu.at[:, pl.ds(0, 128)]), load(eu_h, egu.at[:, pl.ds(128, 128)])]

    for c in l_db:
        c.wait()
    dims = (((1,), (1,)), ((), ()))
    dpre = lax.dot_general(normed, db[0], dims, preferred_element_type=F32)
    bpre = lax.dot_general(normed, db[1], dims, preferred_element_type=F32)
    lane16 = lax.broadcasted_iota(jnp.int32, dpre.shape, 1)
    decay, beta = [], []
    for h in range(2):
        pick = lane16 == tp * 2 + h
        dp = jnp.sum(jnp.where(pick, dpre, 0.0), axis=1, keepdims=True)
        bp = jnp.sum(jnp.where(pick, bpre, 0.0), axis=1, keepdims=True)
        soft = jnp.maximum(dp, 0.0) + jnp.log(1.0 + jnp.exp(-jnp.abs(dp)))
        decay.append(jnp.exp(-rate[:, h : h + 1] * soft))
        beta.append(1.0 / (1.0 + jnp.exp(-bp)))

    for c in l_info:
        c.wait()
    ex = jnp.exp(lgv[...])
    wrow = prv[...] * ex / (ex[0:1] + ex[1:2])
    idf = idv[...].astype(F32)
    square = (ROWS, ROWS)
    eye24 = lax.broadcasted_iota(jnp.int32, square, 0) == lax.broadcasted_iota(jnp.int32, square, 1)

    def column(row):
        return jnp.sum(jnp.where(eye24, jnp.broadcast_to(row, square), 0.0), axis=1, keepdims=True)

    id0, id1 = column(idf[0:1]), column(idf[1:2])
    w0, w1 = column(wrow[0:1]), column(wrow[1:2])
    lanef = lax.broadcasted_iota(jnp.int32, (ROWS, 128), 1).astype(F32)
    rowi = lax.broadcasted_iota(jnp.int32, (ROWS, 128), 0)
    oh = jnp.where((lanef == id0) | (lanef == id1), 1.0, 0.0)
    rank = jnp.zeros((ROWS, 128), F32)
    for i in range(ROWS - 1):
        rank = rank + jnp.where(rowi > i, oh[i : i + 1, :], 0.0)
    table = (rank + 1.0) * oh
    for idk, wk in ((id0, w0), (id1, w1)):
        whi = wk.astype(BF16).astype(F32)
        table = table + jnp.where(lanef == idk + 32.0, whi, 0.0)
        table = table + jnp.where(lanef == idk + 64.0, wk - whi, 0.0)
    rout[z] = table.astype(BF16)

    r_w = [gather_relay(wqkv.at[0], s_w, *g_w[0])]
    c_v = exchange(X_ORDER, at_x, lambda d: wqkv.at[2, x], wqkv.at[2, x], wqkv.at[2, pl.ds(0, 3)])
    r_w.append(gather_relay(wqkv.at[1], s_w, *g_w[1]))
    c_spread.wait_recv()
    i = new("send")
    c_share = send(act.at[core], act.at[core], i, new("recv"), mate)
    leaves(act.at[core], i)
    for c in r_w[0]:
        c.wait_recv()
    ntok = NZ * ROWS

    def half(m, h):
        return jnp.dot(
            act[h].reshape(ntok, 256), wqkv[m, pl.ds(h * 2, 2)].reshape(256, 256), preferred_element_type=F32)

    c_p = []
    for m in range(3):
        if m:
            for c in r_w[m]:
                c.wait_recv()
        part = half(m, core)
        if m == 0:
            c_share.wait_recv()
        part = part + half(m, other)
        psrc[m] = part.astype(BF16).reshape(NZ, ROWS, 2 * HEAD)
        c_p.append(exchange(
            Z_ORDER, at_z, lambda d: psrc.at[m, lax.rem(z + d, NZ)], pdst.at[m, z], pdst.at[m, pl.ds(0, NZ - 1)]))
        pdst[m, z] = psrc[m, z]
        if m == 0:
            r_w.append([c_v])
    for c in l_gu:
        c.wait()
    l_dn.wait()
    s_gu, s_dn = new("send"), new("send")
    g_gu = gather_start(wgu, s_gu)
    g_dn = gather_start(wdn, s_dn)
    leaves(wgu.at[pl.ds(0, 3)], s_gu)
    leaves(wdn.at[pl.ds(0, 3)], s_dn)

    c_r = exchange(Z_ORDER, at_z, lambda d: rout.at[z], rout.at[z], rout.at[pl.ds(0, NZ - 1)])

    def arrived(m):
        c_p[m].wait_recv()
        total = pdst[m, 0].astype(F32)
        for b in range(1, NZ):
            total = total + pdst[m, b].astype(F32)
        return total.astype(BF16).astype(F32)

    def unit(rows):
        return rows * lax.rsqrt(jnp.sum(rows * rows, axis=1, keepdims=True) + EPS)

    def read_state(h, cols):
        return jnp.concatenate(
            [jnp.sum(state[b, h] * cols[:, b : b + 1], axis=0, keepdims=True) for b in range(ROWS)], axis=0)

    l_state.wait()
    rows_k = arrived(0)
    ku = [unit(rows_k[:, h * HEAD : (h + 1) * HEAD]) for h in range(2)]
    kT = [u.T for u in ku]
    rec = [read_state(h, kT[h]) for h in range(2)]
    rows_q = arrived(1)
    qu = [unit(rows_q[:, h * HEAD : (h + 1) * HEAD]) * HEAD ** (-0.5) for h in range(2)]
    red = [read_state(h, qu[h].T) for h in range(2)]
    for c in l_small:
        c.wait()
    l_wo.wait()
    rows_v = arrived(2)
    heads, corrs = [], []
    for h in range(2):
        kq = jnp.sum(ku[h] * qu[h], axis=1, keepdims=True)
        corr = beta[h] * (rows_v[:, h * HEAD : (h + 1) * HEAD] - decay[h] * rec[h])
        ro = decay[h] * red[h] + kq * corr
        ro = ro * lax.rsqrt(jnp.mean(ro * ro, axis=1, keepdims=True) + EPS) * hgain[...]
        heads.append(ro.astype(BF16))
        corrs.append(corr)

    hcat = jnp.concatenate(heads, axis=1)
    si, ri = new("send"), new("recv")
    for d in T_ORDER + ((0, 0),):
        td = t_index(d)
        cols = wo[:, pl.ds(pl.multiple_of(td * SL, SL), SL)]
        asrc[td] = jnp.dot(hcat, cols, preferred_element_type=F32).astype(BF16)
        if d != (0, 0):
            send(asrc.at[td], adst.at[tp], si, ri, at_t(d))
    whole = adst.at[pl.ds(0, NT - 1)]
    leaves(whole, si)
    c_a = remote(whole, whole, ssem.at[si], rsem.at[ri], mate)
    adst[tp] = asrc[tp]

    for h in range(2):
        for b in range(ROWS):
            state[b, h] = state[b, h] * decay[h][b : b + 1, :] + kT[h][:, b : b + 1] * corrs[h][b : b + 1, :]
    w_state = pltpu.make_async_copy(state, state_o, lsem.at[len(local)])
    w_state.start()

    c_a.wait_recv()
    asum = adst[0].astype(F32)
    for b in range(1, NT):
        asum = asum + adst[b].astype(F32)
    middle = tokf[...].astype(F32) + asum
    ss = jnp.sum(middle * middle, axis=1, keepdims=True)
    eye = lax.broadcasted_iota(jnp.int32, (ROWS, 128), 0) == lax.broadcasted_iota(jnp.int32, (ROWS, 128), 1)
    ssb[tp] = jnp.sum(jnp.where(eye, ss, 0.0), axis=0, keepdims=True)
    c_s = exchange(T_ORDER, at_t, lambda d: ssb.at[tp], ssb.at[tp], ssb.at[pl.ds(0, NT - 1)])
    xall[z] = (middle * fgain[...]).astype(BF16)
    c_x = exchange(Z_ORDER, at_z, lambda d: xall.at[z], xall.at[z], xall.at[pl.ds(0, NZ - 1)])
    r_gu = gather_relay(wgu, s_gu, *g_gu)
    r_dn = gather_relay(wdn, s_dn, *g_dn)
    c_s.wait_recv()
    srow = ssb[0]
    for b in range(1, NT):
        srow = srow + ssb[b]
    rsb[z] = lax.rsqrt(srow * (1.0 / D) + EPS)
    c_q = exchange(Z_ORDER, at_z, lambda d: rsb.at[z], rsb.at[z], rsb.at[pl.ds(0, NZ - 1)])

    c_r.wait_recv()
    rt = rout[...].astype(F32)
    shape3 = (NZ, ROWS, 128)
    lane3 = lax.broadcasted_iota(jnp.int32, shape3, 2)
    blk3 = lax.broadcasted_iota(jnp.int32, shape3, 0)
    sel = jnp.zeros(shape3, F32)
    hi = jnp.zeros(shape3, F32)
    lo = jnp.zeros(shape3, F32)
    for xx in range(NX):
        e = z * NX + xx
        r = jnp.sum(jnp.where(lane3 == e, rt, 0.0), axis=2, keepdims=True)
        wh = jnp.sum(jnp.where(lane3 == e + 32, rt, 0.0), axis=2, keepdims=True)
        wl = jnp.sum(jnp.where(lane3 == e + 64, rt, 0.0), axis=2, keepdims=True)
        place = blk3.astype(F32) * CAP + (r - 1.0) + float(xx * SLOTS)
        hit = (lane3.astype(F32) == place) & (r > 0.5)
        sel = sel + jnp.where(hit, 1.0, 0.0)
        hi = hi + jnp.where(hit, wh, 0.0)
        lo = lo + jnp.where(hit, wl, 0.0)
    selT = sel.reshape(ntok, 128).T.astype(BF16)
    hi2 = hi.reshape(ntok, 128).astype(BF16)
    lo2 = lo.reshape(ntok, 128).astype(BF16)

    c_x.wait_recv()
    xs2 = xall[...].reshape(ntok, SL)
    picked = jnp.dot(selT, xs2, preferred_element_type=F32).astype(BF16)
    for xx in range(NX):
        esrc[xx] = picked[xx * SLOTS : (xx + 1) * SLOTS]
    si = new("send")
    r_e = {d: new("recv") for d in (0,) + Y_ORDER}
    for dx, dy in E_ORDER:
        xd = lax.rem(x + dx, NX)
        dev = {"ep": z * NX + xd, "tp": y_index(dy)}
        send(esrc.at[xd], eall.at[tp, x], si, r_e[dy], dev)
    leaves(eall.at[pl.ds(0, 3)], si)
    leaves_e = eall.at[0, pl.ds(0, NX - 1)]
    leaves(leaves_e, si)
    eall[tp, x] = esrc[x]

    for c in r_gu:
        c.wait_recv()
    for xx in range(NX):
        part = jnp.dot(xs2, wgu[xx], preferred_element_type=F32).astype(BF16).reshape(NZ, ROWS, 256)
        for b in range(NZ):
            dsrc[b % 2, b // 2, :, xx * 256 : (xx + 1) * 256] = part[b]
    c_q.wait_recv()
    eye3 = lax.broadcasted_iota(jnp.int32, shape3, 1) == lane3
    rcol = jnp.sum(jnp.where(eye3, jnp.broadcast_to(rsb[...], shape3), 0.0), axis=2, keepdims=True)
    rhi = rcol.astype(BF16).astype(F32)
    pair = jnp.where(lane3 < 64, rhi, rcol - rhi).astype(BF16).reshape(ntok, 128)
    rslot = jnp.dot(selT, pair, preferred_element_type=F32)
    rslot = jnp.broadcast_to(rslot[:, 0:1] + rslot[:, 127:128], (128, 128))
    for xx in range(NX):
        qsrc[xx] = rslot[xx * SLOTS : (xx + 1) * SLOTS]
    c_sc = exchange(
        X_ORDER, at_x, lambda d: qsrc.at[lax.rem(x + d, NX)], qdst.at[x], qdst.at[pl.ds(0, NX - 1)])
    qdst[x] = qsrc[x]
    i = new("send")
    c_dm = send(dsrc.at[other], dmate, i, new("recv"), mate)
    leaves(dmate, i)
    for c in l_egu:
        c.wait()
    c_dm.wait_recv()
    for b in range(NY):
        dpair[b] = (dsrc[core, b].astype(F32) + dmate[b].astype(F32)).astype(BF16)
    c_d = exchange(
        Y_ORDER, at_y, lambda d: dpair.at[lax.rem(y + d, NY)], ddst.at[y], ddst.at[pl.ds(0, NY - 1)])
    ddst[y] = dpair[y]

    def hidden_part(t):
        rows = egu[pl.ds(pl.multiple_of(t * SL, SL), SL), :]
        return jnp.dot(eall[t].reshape(NX * SLOTS, SL), rows, preferred_element_type=F32)

    s_m = new("send")
    acc = jnp.zeros((NX * SLOTS, 256), F32)
    c_m = []
    for dy in (0, 1, 3, 2):
        t = y_index(NY - dy)
        got = eall.at[t] if dy else leaves_e
        remote(got, got, ssem.at[si], rsem.at[r_e[dy]], mate).wait_recv()
        c_m.append(send(eall.at[t], eall.at[t], s_m, new("recv"), mate))
        acc = acc + hidden_part(t)
    leaves(eall.at[pl.ds(0, NY)], s_m)
    for c, dy in zip(c_m, (0, 1, 3, 2)):
        c.wait_recv()
        acc = acc + hidden_part(lax.rem(y + NY - dy, NY) * 2 + other)

    def tp_gather(buf):
        si, rm = new("send"), new("recv")
        out = [send(buf.at[tp], buf.at[tp], si, new("recv"), at_y(d)) for d in Y_ORDER]
        send(buf.at[tp], buf.at[tp], si, rm, mate)
        return si, rm, out

    def tp_hand_on(buf, si, rm, out):
        for c, d in zip(out, Y_ORDER):
            c.wait_recv()
            t = y_index(NY - d)
            send(buf.at[t], buf.at[t], si, rm, mate)
        leaves(buf.at[pl.ds(0, NT - 1)], si)
        got = buf.at[pl.ds(0, NY)]
        return remote(got, got, ssem.at[si], rsem.at[rm], mate)

    c_sc.wait_recv()
    scale = qdst[...].reshape(NX * SLOTS, 128)
    ga, ua = acc[:, :128] * scale, acc[:, 128:] * scale
    ehall[tp] = (ga / (1.0 + jnp.exp(-ga)) * ua).astype(BF16)
    c_eh = tp_gather(ehall)

    c_d.wait_recv()
    dsum = ddst[0].astype(F32)
    for b in range(1, NY):
        dsum = dsum + ddst[b].astype(F32)
    dsum = dsum * jnp.sum(jnp.where(eye, jnp.broadcast_to(rsb[tp], (ROWS, 128)), 0.0), axis=1, keepdims=True)
    hid = []
    for xx in range(NX):
        g = dsum[:, xx * 256 : xx * 256 + 128]
        u = dsum[:, xx * 256 + 128 : xx * 256 + 256]
        hid.append((g / (1.0 + jnp.exp(-g)) * u).astype(BF16))
    hall[tp] = jnp.concatenate(hid, axis=1)
    c_h = tp_gather(hall)

    l_ed.wait()
    c_ed.wait_recv()
    c_eh = tp_hand_on(ehall, *c_eh)
    c_h = tp_hand_on(hall, *c_h)
    c_eh.wait_recv()
    eres = jnp.zeros((NX * SLOTS, SL), F32)
    for t in range(NT):
        eres = eres + jnp.dot(ehall[t], edn[t], preferred_element_type=F32)
    rsrc[...] = eres.astype(BF16).reshape(NX, SLOTS, SL)
    c_b = exchange(
        X_ORDER, at_x, lambda d: rsrc.at[lax.rem(x + d, NX)], rdst.at[x], rdst.at[pl.ds(0, NX - 1)])
    rdst[x] = rsrc[x]

    for c in r_dn:
        c.wait_recv()
    c_h.wait_recv()
    down = jnp.dot(
        hall[...].reshape(ntok, SL), wdn[...].reshape(SL, SL), preferred_element_type=F32)
    down = down * (1.0 / (1.0 + jnp.exp(-mixv[...])))
    c_b.wait_recv()
    back = rdst[...].reshape(NX * SLOTS, SL)
    down = down + jnp.dot(hi2[:, : NX * SLOTS], back, preferred_element_type=F32)
    down = down + jnp.dot(lo2[:, : NX * SLOTS], back, preferred_element_type=F32)
    fsrc[...] = down.astype(BF16).reshape(NZ, ROWS, SL)
    c_f = exchange(
        Z_ORDER, at_z, lambda d: fsrc.at[lax.rem(z + d, NZ)], fdst.at[z], fdst.at[pl.ds(0, NZ - 1)])
    fdst[z] = fsrc[z]
    c_f.wait_recv()
    total = middle
    for b in range(NZ):
        total = total + fdst[b].astype(F32)
    out_ref[...] = total.astype(BF16)

    for c in last:
        c.wait_send()
    w_state.wait()
    assert count == {"send": N_SEND, "recv": N_RECV}, count


def per_device(
    tokens, delta_state, attn_gain, query_weight, key_weight, value_weight, decay_weight, beta_weight, decay_rate,
    head_gain, output_weight, ffn_gain, expert_ids, group_prob, expert_logit, expert_gate, expert_up, expert_down,
    dense_gate, dense_up, dense_down, dense_mix,
):
    hbm = pl.BlockSpec(memory_space=pltpu.HBM)
    in_specs = [hbm] * 22
    vm = pltpu.VMEM
    scratch = [
        vm((ROWS, D), BF16), vm((ROWS, SL), BF16), vm((1, D), F32), vm((3, NX, 128, 256), BF16), vm((2, 16, D), BF16),
        vm((1, 2), F32),        vm((1, HEAD), F32), vm((256, D), BF16), vm((1, SL), F32), vm((2, ROWS), jnp.int32),
        vm((2, ROWS), F32), vm((1, ROWS), F32), vm((NX, SL, 256), BF16), vm((NX, 128, SL), BF16), vm((1, SL), F32), vm((D, 256), BF16), vm((NT, 128, SL), BF16),
        vm((ROWS, 2, HEAD, HEAD), F32),
        vm((2, NZ, ROWS, 256), BF16), vm((2, NZ, ROWS, 256), BF16),
        vm((3, NZ, ROWS, 256), BF16), vm((3, NZ, ROWS, 256), BF16), vm((NZ, ROWS, 128), BF16),
        vm((NT, ROWS, SL), BF16), vm((NT, ROWS, SL), BF16), vm((NT, 1, 128), F32), vm((NZ, 1, 128), F32),
        vm((NZ, ROWS, SL), BF16),
        vm((2, NY, ROWS, 1024), BF16), vm((NY, ROWS, 1024), BF16), vm((NY, ROWS, 1024), BF16),
        vm((NY, ROWS, 1024), BF16), vm((NX, SLOTS, 128), F32), vm((NX, SLOTS, 128), F32), vm((NT, ROWS, SL), BF16),
        vm((NX, SLOTS, SL), BF16), vm((NT, NX, SLOTS, SL), BF16), vm((NT, NX * SLOTS, 128), BF16),
        vm((NX, SLOTS, SL), BF16), vm((NX, SLOTS, SL), BF16), vm((NZ, ROWS, SL), BF16), vm((NZ, ROWS, SL), BF16),
        pltpu.SemaphoreType.DMA((32,)),
        pltpu.SemaphoreType.DMA((N_SEND,)), pltpu.SemaphoreType.DMA((N_RECV,)),
    ]
    operands = (
        tokens, delta_state, attn_gain.reshape(1, D), query_weight, key_weight, value_weight, decay_weight.T,
        beta_weight.T, decay_rate.reshape(1, 2), head_gain.reshape(1, HEAD), output_weight, ffn_gain.reshape(1, D), expert_ids.T,
        expert_logit.T, group_prob.reshape(1, ROWS), expert_gate.reshape(D, 128), expert_up.reshape(D, 128),
        expert_down.reshape(128, D), dense_gate, dense_up, dense_down, dense_mix.reshape(1, SL),
    )
    operands = [pltpu.with_memory_space_constraint(o, pltpu.HBM) for o in operands]
    mixed_out, new_state = pl.pallas_call(
        kernel,
        out_shape=(
            jax.ShapeDtypeStruct((ROWS, SL), BF16),
            jax.ShapeDtypeStruct((ROWS, 2, HEAD, HEAD), F32),
        ),
        in_specs=in_specs,
        out_specs=(pl.BlockSpec(memory_space=pltpu.VMEM), pl.BlockSpec(memory_space=pl.ANY)),
        scratch_shapes=scratch,
        compiler_params=pltpu.CompilerParams(
            collective_id=0, has_side_effects=True, vmem_limit_bytes=24 * 1024 * 1024),
        name="layer",
    )(*operands)
    return mixed_out, new_state


def solution(mesh):
    return jax.shard_map(
        per_device,
        mesh=mesh,
        in_specs=(
            P("ep", None),
            P("ep", "tp", None, None),
            P(),
            P("ep", "tp"),
            P("ep", "tp"),
            P("ep", "tp"),
            P(),
            P(),
            P("tp"),
            P(),
            P("tp", None),
            P(),
            P("ep", None),
            P("ep"),
            P("ep", None),
            P("ep", None, "tp"),
            P("ep", None, "tp"),
            P("ep", "tp", None),
            P("tp", "ep"),
            P("tp", "ep"),
            P("ep", "tp"),
            P("tp"),
        ),
        out_specs=(P("ep", "tp"), P("ep", "tp", None, None)),
        check_vma=False,
    )
```

```python
import jax
import jax.numpy as jnp
from jax import lax
from jax.experimental import pallas as pl
from jax.experimental.pallas import tpu as pltpu
from jax.sharding import PartitionSpec as P

EPS = 1e-06
MESH = pl.DeviceIdType.MESH
F32 = jnp.float32
BF16 = jnp.bfloat16

NX, NZ, NY, NT = 4, 8, 4, 8
ROWS = 24
D = 4096
SL = 512
HEAD = 128
CAP = 3
SLOTS = NZ * CAP
N_SEND, N_RECV = 24, 43
X_ORDER = (2, 1, 3)
Z_ORDER = (4, 3, 5, 2, 6, 1, 7)
Y_ORDER = (2, 1, 3)
E_ORDER = tuple(
    (dx, dy) for far in (4, 3, 2, 1) for dy in Y_ORDER + (0,) for dx in X_ORDER + (0,)
    if min(dx, NX - dx) + min(dy, NY - dy) == far)
T_ORDER = ((2, 0), (2, 1), (1, 0), (1, 1), (3, 0), (3, 1), (0, 1))


def kernel(
    tok_h, state_h, again_h, wq_h, wk_h, wv_h, dT_h, bT_h, rate_h, hgain_h, wo_h, fgain_h, ids_h,
    lgt_h, prob_h,
    eg_h, eu_h, ed_h, dg_h, du_h, dd_h, mix_h,
    out_ref, state_o,
    tok, tokf, again, wqkv, db, rate, hgain, wo, fgain, idv, lgv, prv, wgu, wdn, mixv, egu, edn, state,
    spread, act, psrc, pdst, rout, asrc, adst, ssb, rsb, xall, dsrc, dmate, dpair, ddst, qsrc, qdst, hall, esrc, eall, ehall, rsrc, rdst, fsrc, fdst,
    lsem, ssem, rsem,
):
    ep = lax.axis_index("ep")
    tp = lax.axis_index("tp")
    z = ep // NX
    x = lax.rem(ep, NX)

    def at_x(d):
        return {"ep": z * NX + lax.rem(x + d, NX), "tp": tp}

    def at_z(d):
        return {"ep": lax.rem(z + d, NZ) * NX + x, "tp": tp}

    y = tp // 2
    core = lax.rem(tp, 2)

    def t_index(d):
        return lax.rem(y + d[0], NY) * 2 + lax.rem(core + d[1], 2)

    def at_t(d):
        return {"ep": ep, "tp": t_index(d)}

    other = 1 - core
    mate = {"ep": ep, "tp": y * 2 + other}

    def y_index(d):
        return lax.rem(y + d, NY) * 2 + core

    def at_y(d):
        return {"ep": ep, "tp": y_index(d)}

    def remote(src, dst, ss, rs, dev):
        return pltpu.make_async_remote_copy(
            src_ref=src, dst_ref=dst, send_sem=ss, recv_sem=rs, device_id=dev, device_id_type=MESH
        )

    count = {"send": 0, "recv": 0}
    last = []

    def new(kind):
        count[kind] += 1
        return count[kind] - 1

    def send(src, dst, si, ri, dev):
        copy = remote(src, dst, ssem.at[si], rsem.at[ri], dev)
        copy.start()
        return copy

    def leaves(whole, si):
        last.append(remote(whole, whole, ssem.at[si], rsem.at[0], mate))

    def exchange(order, at, src, dst, whole):
        si, ri = new("send"), new("recv")
        for d in order:
            send(src(d), dst, si, ri, at(d))
        leaves(whole, si)
        return remote(whole, whole, ssem.at[si], rsem.at[ri], mate)

    local = []

    def load(src, dst):
        c = pltpu.make_async_copy(src, dst, lsem.at[len(local)])
        c.start()
        local.append(c)
        return c

    bar = pltpu.get_barrier_semaphore()
    for d in X_ORDER:
        pl.semaphore_signal(bar, inc=1, device_id=at_x(d), device_id_type=MESH)
    for d in Z_ORDER:
        pl.semaphore_signal(bar, inc=1, device_id=at_z(d), device_id_type=MESH)
    for d in T_ORDER:
        pl.semaphore_signal(bar, inc=1, device_id=at_t(d), device_id_type=MESH)

    l_tok = load(tok_h, tok)
    l_again = load(again_h, again)
    l_w = [load(w, wqkv.at[m, x]) for m, w in enumerate((wk_h, wq_h, wv_h))]

    pl.semaphore_wait(bar, NX + NZ + NT - 3)

    left = lax.rem(x + NX - 1, NX)
    right = lax.rem(x + 1, NX)

    def gather_start(buf, si):
        return (
            send(buf.at[x], buf.at[x], si, new("recv"), at_x(1)),
            send(buf.at[x], buf.at[x], si, new("recv"), at_x(NX - 1)),
        )

    def gather_relay(buf, si, c0, c1):
        h = buf.shape[1] // 2
        low, high = buf.at[left, pl.ds(0, h)], buf.at[right, pl.ds(h, h)]
        c0.wait_recv()
        r0 = send(low, low, si, new("recv"), at_x(1))
        c1.wait_recv()
        r1 = send(high, high, si, new("recv"), at_x(NX - 1))
        return r0, r1

    for c in l_w:
        c.wait()
    s_w = new("send")
    leaves(wqkv.at[pl.ds(0, 2), pl.ds(0, 3)], s_w)
    g_w = [gather_start(wqkv.at[m], s_w) for m in range(2)]

    l_tok.wait()
    l_again.wait()
    t32 = tok[...].astype(F32)
    ms = jnp.sum(t32 * t32, axis=1, keepdims=True) * (1.0 / D)
    normed = (t32 * lax.rsqrt(ms + EPS) * again[...]).astype(BF16)
    for b in range(NZ):
        for h in range(2):
            spread[h, b] = normed[:, b * SL + h * 256 : b * SL + (h + 1) * 256]

    c_spread = exchange(
        Z_ORDER, at_z, lambda d: spread.at[core, lax.rem(z + d, NZ)], act.at[core, z], act.at[core, pl.ds(0, NZ - 1)])
    act[core, z] = spread[core, z]

    c_ed = exchange(
        T_ORDER, at_t, lambda d: ed_h.at[:, pl.ds(pl.multiple_of(t_index(d) * SL, SL), SL)], edn.at[tp],
        edn.at[pl.ds(0, NT - 1)])

    l_db = [load(dT_h, db.at[0]), load(bT_h, db.at[1]), load(rate_h, rate)]
    l_info = [load(ids_h, idv), load(lgt_h, lgv), load(prob_h, prv)]
    l_gu = [load(dg_h, wgu.at[x, :, pl.ds(0, 128)]), load(du_h, wgu.at[x, :, pl.ds(128, 128)])]
    l_dn = load(dd_h, wdn.at[x])
    l_state = load(state_h, state)
    l_wo = load(wo_h, wo)
    l_small = [
        load(hgain_h, hgain),
        load(fgain_h.at[:, pl.ds(pl.multiple_of(tp * SL, SL), SL)], fgain),
        load(mix_h, mixv),
        load(tok_h.at[:, pl.ds(pl.multiple_of(tp * SL, SL), SL)], tokf),
    ]
    l_ed = load(ed_h.at[:, pl.ds(pl.multiple_of(tp * SL, SL), SL)], edn.at[tp])
    l_egu = [load(eg_h, egu.at[:, pl.ds(0, 128)]), load(eu_h, egu.at[:, pl.ds(128, 128)])]

    for c in l_db:
        c.wait()
    dims = (((1,), (1,)), ((), ()))
    dpre = lax.dot_general(normed, db[0], dims, preferred_element_type=F32)
    bpre = lax.dot_general(normed, db[1], dims, preferred_element_type=F32)
    lane16 = lax.broadcasted_iota(jnp.int32, dpre.shape, 1)
    decay, beta = [], []
    for h in range(2):
        pick = lane16 == tp * 2 + h
        dp = jnp.sum(jnp.where(pick, dpre, 0.0), axis=1, keepdims=True)
        bp = jnp.sum(jnp.where(pick, bpre, 0.0), axis=1, keepdims=True)
        soft = jnp.maximum(dp, 0.0) + jnp.log(1.0 + jnp.exp(-jnp.abs(dp)))
        decay.append(jnp.exp(-rate[:, h : h + 1] * soft))
        beta.append(1.0 / (1.0 + jnp.exp(-bp)))

    for c in l_info:
        c.wait()
    ex = jnp.exp(lgv[...])
    wrow = prv[...] * ex / (ex[0:1] + ex[1:2])
    idf = idv[...].astype(F32)
    square = (ROWS, ROWS)
    eye24 = lax.broadcasted_iota(jnp.int32, square, 0) == lax.broadcasted_iota(jnp.int32, square, 1)

    def column(row):
        return jnp.sum(jnp.where(eye24, jnp.broadcast_to(row, square), 0.0), axis=1, keepdims=True)

    id0, id1 = column(idf[0:1]), column(idf[1:2])
    w0, w1 = column(wrow[0:1]), column(wrow[1:2])
    lanef = lax.broadcasted_iota(jnp.int32, (ROWS, 128), 1).astype(F32)
    rowi = lax.broadcasted_iota(jnp.int32, (ROWS, 128), 0)
    oh = jnp.where((lanef == id0) | (lanef == id1), 1.0, 0.0)
    rank = jnp.zeros((ROWS, 128), F32)
    for i in range(ROWS - 1):
        rank = rank + jnp.where(rowi > i, oh[i : i + 1, :], 0.0)
    table = (rank + 1.0) * oh
    for idk, wk in ((id0, w0), (id1, w1)):
        whi = wk.astype(BF16).astype(F32)
        table = table + jnp.where(lanef == idk + 32.0, whi, 0.0)
        table = table + jnp.where(lanef == idk + 64.0, wk - whi, 0.0)
    rout[z] = table.astype(BF16)

    r_w = [gather_relay(wqkv.at[0], s_w, *g_w[0])]
    c_v = exchange(X_ORDER, at_x, lambda d: wqkv.at[2, x], wqkv.at[2, x], wqkv.at[2, pl.ds(0, 3)])
    r_w.append(gather_relay(wqkv.at[1], s_w, *g_w[1]))
    c_spread.wait_recv()
    i = new("send")
    c_share = send(act.at[core], act.at[core], i, new("recv"), mate)
    leaves(act.at[core], i)
    for c in r_w[0]:
        c.wait_recv()
    ntok = NZ * ROWS

    def half(m, h):
        return jnp.dot(
            act[h].reshape(ntok, 256), wqkv[m, pl.ds(h * 2, 2)].reshape(256, 256), preferred_element_type=F32)

    c_p = []
    for m in range(3):
        if m:
            for c in r_w[m]:
                c.wait_recv()
        part = half(m, core)
        if m == 0:
            c_share.wait_recv()
        part = part + half(m, other)
        psrc[m] = part.astype(BF16).reshape(NZ, ROWS, 2 * HEAD)
        c_p.append(exchange(
            Z_ORDER, at_z, lambda d: psrc.at[m, lax.rem(z + d, NZ)], pdst.at[m, z], pdst.at[m, pl.ds(0, NZ - 1)]))
        pdst[m, z] = psrc[m, z]
        if m == 0:
            r_w.append([c_v])
    for c in l_gu:
        c.wait()
    l_dn.wait()
    s_gu, s_dn = new("send"), new("send")
    g_gu = gather_start(wgu, s_gu)
    g_dn = gather_start(wdn, s_dn)
    leaves(wgu.at[pl.ds(0, 3)], s_gu)
    leaves(wdn.at[pl.ds(0, 3)], s_dn)

    c_r = exchange(Z_ORDER, at_z, lambda d: rout.at[z], rout.at[z], rout.at[pl.ds(0, NZ - 1)])

    def arrived(m):
        c_p[m].wait_recv()
        total = pdst[m, 0].astype(F32)
        for b in range(1, NZ):
            total = total + pdst[m, b].astype(F32)
        return total.astype(BF16).astype(F32)

    def unit(rows):
        return rows * lax.rsqrt(jnp.sum(rows * rows, axis=1, keepdims=True) + EPS)

    def read_state(h, cols):
        return jnp.concatenate(
            [jnp.sum(state[b, h] * cols[:, b : b + 1], axis=0, keepdims=True) for b in range(ROWS)], axis=0)

    l_state.wait()
    rows_k = arrived(0)
    ku = [unit(rows_k[:, h * HEAD : (h + 1) * HEAD]) for h in range(2)]
    kT = [u.T for u in ku]
    rec = [read_state(h, kT[h]) for h in range(2)]
    rows_q = arrived(1)
    qu = [unit(rows_q[:, h * HEAD : (h + 1) * HEAD]) * HEAD ** (-0.5) for h in range(2)]
    red = [read_state(h, qu[h].T) for h in range(2)]
    for c in l_small:
        c.wait()
    l_wo.wait()
    rows_v = arrived(2)
    heads, corrs = [], []
    for h in range(2):
        kq = jnp.sum(ku[h] * qu[h], axis=1, keepdims=True)
        corr = beta[h] * (rows_v[:, h * HEAD : (h + 1) * HEAD] - decay[h] * rec[h])
        ro = decay[h] * red[h] + kq * corr
        ro = ro * lax.rsqrt(jnp.mean(ro * ro, axis=1, keepdims=True) + EPS) * hgain[...]
        heads.append(ro.astype(BF16))
        corrs.append(corr)

    hcat = jnp.concatenate(heads, axis=1)
    si, ri = new("send"), new("recv")
    for d in T_ORDER + ((0, 0),):
        td = t_index(d)
        cols = wo[:, pl.ds(pl.multiple_of(td * SL, SL), SL)]
        asrc[td] = jnp.dot(hcat, cols, preferred_element_type=F32).astype(BF16)
        if d != (0, 0):
            send(asrc.at[td], adst.at[tp], si, ri, at_t(d))
    whole = adst.at[pl.ds(0, NT - 1)]
    leaves(whole, si)
    c_a = remote(whole, whole, ssem.at[si], rsem.at[ri], mate)
    adst[tp] = asrc[tp]

    for h in range(2):
        for b in range(ROWS):
            state[b, h] = state[b, h] * decay[h][b : b + 1, :] + kT[h][:, b : b + 1] * corrs[h][b : b + 1, :]
    w_state = pltpu.make_async_copy(state, state_o, lsem.at[len(local)])
    w_state.start()

    c_a.wait_recv()
    asum = adst[0].astype(F32)
    for b in range(1, NT):
        asum = asum + adst[b].astype(F32)
    middle = tokf[...].astype(F32) + asum
    ss = jnp.sum(middle * middle, axis=1, keepdims=True)
    eye = lax.broadcasted_iota(jnp.int32, (ROWS, 128), 0) == lax.broadcasted_iota(jnp.int32, (ROWS, 128), 1)
    ssb[tp] = jnp.sum(jnp.where(eye, ss, 0.0), axis=0, keepdims=True)
    c_s = exchange(T_ORDER, at_t, lambda d: ssb.at[tp], ssb.at[tp], ssb.at[pl.ds(0, NT - 1)])
    xall[z] = (middle * fgain[...]).astype(BF16)
    c_x = exchange(Z_ORDER, at_z, lambda d: xall.at[z], xall.at[z], xall.at[pl.ds(0, NZ - 1)])
    r_gu = gather_relay(wgu, s_gu, *g_gu)
    r_dn = gather_relay(wdn, s_dn, *g_dn)
    c_s.wait_recv()
    srow = ssb[0]
    for b in range(1, NT):
        srow = srow + ssb[b]
    rsb[z] = lax.rsqrt(srow * (1.0 / D) + EPS)
    c_q = exchange(Z_ORDER, at_z, lambda d: rsb.at[z], rsb.at[z], rsb.at[pl.ds(0, NZ - 1)])

    c_r.wait_recv()
    rt = rout[...].astype(F32)
    shape3 = (NZ, ROWS, 128)
    lane3 = lax.broadcasted_iota(jnp.int32, shape3, 2)
    blk3 = lax.broadcasted_iota(jnp.int32, shape3, 0)
    sel = jnp.zeros(shape3, F32)
    hi = jnp.zeros(shape3, F32)
    lo = jnp.zeros(shape3, F32)
    for xx in range(NX):
        e = z * NX + xx
        r = jnp.sum(jnp.where(lane3 == e, rt, 0.0), axis=2, keepdims=True)
        wh = jnp.sum(jnp.where(lane3 == e + 32, rt, 0.0), axis=2, keepdims=True)
        wl = jnp.sum(jnp.where(lane3 == e + 64, rt, 0.0), axis=2, keepdims=True)
        place = blk3.astype(F32) * CAP + (r - 1.0) + float(xx * SLOTS)
        hit = (lane3.astype(F32) == place) & (r > 0.5)
        sel = sel + jnp.where(hit, 1.0, 0.0)
        hi = hi + jnp.where(hit, wh, 0.0)
        lo = lo + jnp.where(hit, wl, 0.0)
    selT = sel.reshape(ntok, 128).T.astype(BF16)
    hi2 = hi.reshape(ntok, 128).astype(BF16)
    lo2 = lo.reshape(ntok, 128).astype(BF16)

    c_x.wait_recv()
    xs2 = xall[...].reshape(ntok, SL)
    picked = jnp.dot(selT, xs2, preferred_element_type=F32).astype(BF16)
    for xx in range(NX):
        esrc[xx] = picked[xx * SLOTS : (xx + 1) * SLOTS]
    si = new("send")
    r_e = {d: new("recv") for d in (0,) + Y_ORDER}
    for dx, dy in E_ORDER:
        xd = lax.rem(x + dx, NX)
        dev = {"ep": z * NX + xd, "tp": y_index(dy)}
        send(esrc.at[xd], eall.at[tp, x], si, r_e[dy], dev)
    leaves(eall.at[pl.ds(0, 3)], si)
    leaves_e = eall.at[0, pl.ds(0, NX - 1)]
    leaves(leaves_e, si)
    eall[tp, x] = esrc[x]

    for c in r_gu:
        c.wait_recv()
    for xx in range(NX):
        part = jnp.dot(xs2, wgu[xx], preferred_element_type=F32).astype(BF16).reshape(NZ, ROWS, 256)
        for b in range(NZ):
            dsrc[b % 2, b // 2, :, xx * 256 : (xx + 1) * 256] = part[b]
    c_q.wait_recv()
    eye3 = lax.broadcasted_iota(jnp.int32, shape3, 1) == lane3
    rcol = jnp.sum(jnp.where(eye3, jnp.broadcast_to(rsb[...], shape3), 0.0), axis=2, keepdims=True)
    rhi = rcol.astype(BF16).astype(F32)
    pair = jnp.where(lane3 < 64, rhi, rcol - rhi).astype(BF16).reshape(ntok, 128)
    rslot = jnp.dot(selT, pair, preferred_element_type=F32)
    rslot = jnp.broadcast_to(rslot[:, 0:1] + rslot[:, 127:128], (128, 128))
    for xx in range(NX):
        qsrc[xx] = rslot[xx * SLOTS : (xx + 1) * SLOTS]
    c_sc = exchange(
        X_ORDER, at_x, lambda d: qsrc.at[lax.rem(x + d, NX)], qdst.at[x], qdst.at[pl.ds(0, NX - 1)])
    qdst[x] = qsrc[x]
    i = new("send")
    c_dm = send(dsrc.at[other], dmate, i, new("recv"), mate)
    leaves(dmate, i)
    for c in l_egu:
        c.wait()
    c_dm.wait_recv()
    for b in range(NY):
        dpair[b] = (dsrc[core, b].astype(F32) + dmate[b].astype(F32)).astype(BF16)
    c_d = exchange(
        Y_ORDER, at_y, lambda d: dpair.at[lax.rem(y + d, NY)], ddst.at[y], ddst.at[pl.ds(0, NY - 1)])
    ddst[y] = dpair[y]

    def hidden_part(t):
        rows = egu[pl.ds(pl.multiple_of(t * SL, SL), SL), :]
        return jnp.dot(eall[t].reshape(NX * SLOTS, SL), rows, preferred_element_type=F32)

    s_m = new("send")
    acc = jnp.zeros((NX * SLOTS, 256), F32)
    c_m = []
    for dy in (0, 1, 3, 2):
        t = y_index(NY - dy)
        got = eall.at[t] if dy else leaves_e
        remote(got, got, ssem.at[si], rsem.at[r_e[dy]], mate).wait_recv()
        c_m.append(send(eall.at[t], eall.at[t], s_m, new("recv"), mate))
        acc = acc + hidden_part(t)
    leaves(eall.at[pl.ds(0, NY)], s_m)
    for c, dy in zip(c_m, (0, 1, 3, 2)):
        c.wait_recv()
        acc = acc + hidden_part(lax.rem(y + NY - dy, NY) * 2 + other)

    def tp_gather(buf):
        return exchange(T_ORDER, at_t, lambda d: buf.at[tp], buf.at[tp], buf.at[pl.ds(0, NT - 1)])

    c_sc.wait_recv()
    scale = qdst[...].reshape(NX * SLOTS, 128)
    ga, ua = acc[:, :128] * scale, acc[:, 128:] * scale
    ehall[tp] = (ga / (1.0 + jnp.exp(-ga)) * ua).astype(BF16)
    c_eh = tp_gather(ehall)

    c_d.wait_recv()
    dsum = ddst[0].astype(F32)
    for b in range(1, NY):
        dsum = dsum + ddst[b].astype(F32)
    dsum = dsum * jnp.sum(jnp.where(eye, jnp.broadcast_to(rsb[tp], (ROWS, 128)), 0.0), axis=1, keepdims=True)
    hid = []
    for xx in range(NX):
        g = dsum[:, xx * 256 : xx * 256 + 128]
        u = dsum[:, xx * 256 + 128 : xx * 256 + 256]
        hid.append((g / (1.0 + jnp.exp(-g)) * u).astype(BF16))
    hall[tp] = jnp.concatenate(hid, axis=1)
    c_h = tp_gather(hall)

    l_ed.wait()
    c_ed.wait_recv()
    c_eh.wait_recv()
    eres = jnp.zeros((NX * SLOTS, SL), F32)
    for t in range(NT):
        eres = eres + jnp.dot(ehall[t], edn[t], preferred_element_type=F32)
    rsrc[...] = eres.astype(BF16).reshape(NX, SLOTS, SL)
    c_b = exchange(
        X_ORDER, at_x, lambda d: rsrc.at[lax.rem(x + d, NX)], rdst.at[x], rdst.at[pl.ds(0, NX - 1)])
    rdst[x] = rsrc[x]

    for c in r_dn:
        c.wait_recv()
    c_h.wait_recv()
    down = jnp.dot(
        hall[...].reshape(ntok, SL), wdn[...].reshape(SL, SL), preferred_element_type=F32)
    down = down * (1.0 / (1.0 + jnp.exp(-mixv[...])))
    c_b.wait_recv()
    back = rdst[...].reshape(NX * SLOTS, SL)
    down = down + jnp.dot(hi2[:, : NX * SLOTS], back, preferred_element_type=F32)
    down = down + jnp.dot(lo2[:, : NX * SLOTS], back, preferred_element_type=F32)
    fsrc[...] = down.astype(BF16).reshape(NZ, ROWS, SL)
    c_f = exchange(
        Z_ORDER, at_z, lambda d: fsrc.at[lax.rem(z + d, NZ)], fdst.at[z], fdst.at[pl.ds(0, NZ - 1)])
    fdst[z] = fsrc[z]
    c_f.wait_recv()
    total = middle
    for b in range(NZ):
        total = total + fdst[b].astype(F32)
    out_ref[...] = total.astype(BF16)

    for c in last:
        c.wait_send()
    w_state.wait()
    assert count == {"send": N_SEND, "recv": N_RECV}, count


def per_device(
    tokens, delta_state, attn_gain, query_weight, key_weight, value_weight, decay_weight, beta_weight, decay_rate,
    head_gain, output_weight, ffn_gain, expert_ids, group_prob, expert_logit, expert_gate, expert_up, expert_down,
    dense_gate, dense_up, dense_down, dense_mix,
):
    hbm = pl.BlockSpec(memory_space=pltpu.HBM)
    in_specs = [hbm] * 22
    vm = pltpu.VMEM
    scratch = [
        vm((ROWS, D), BF16), vm((ROWS, SL), BF16), vm((1, D), F32), vm((3, NX, 128, 256), BF16), vm((2, 16, D), BF16),
        vm((1, 2), F32),        vm((1, HEAD), F32), vm((256, D), BF16), vm((1, SL), F32), vm((2, ROWS), jnp.int32),
        vm((2, ROWS), F32), vm((1, ROWS), F32), vm((NX, SL, 256), BF16), vm((NX, 128, SL), BF16), vm((1, SL), F32), vm((D, 256), BF16), vm((NT, 128, SL), BF16),
        vm((ROWS, 2, HEAD, HEAD), F32),
        vm((2, NZ, ROWS, 256), BF16), vm((2, NZ, ROWS, 256), BF16),
        vm((3, NZ, ROWS, 256), BF16), vm((3, NZ, ROWS, 256), BF16), vm((NZ, ROWS, 128), BF16),
        vm((NT, ROWS, SL), BF16), vm((NT, ROWS, SL), BF16), vm((NT, 1, 128), F32), vm((NZ, 1, 128), F32),
        vm((NZ, ROWS, SL), BF16),
        vm((2, NY, ROWS, 1024), BF16), vm((NY, ROWS, 1024), BF16), vm((NY, ROWS, 1024), BF16),
        vm((NY, ROWS, 1024), BF16), vm((NX, SLOTS, 128), F32), vm((NX, SLOTS, 128), F32), vm((NT, ROWS, SL), BF16),
        vm((NX, SLOTS, SL), BF16), vm((NT, NX, SLOTS, SL), BF16), vm((NT, NX * SLOTS, 128), BF16),
        vm((NX, SLOTS, SL), BF16), vm((NX, SLOTS, SL), BF16), vm((NZ, ROWS, SL), BF16), vm((NZ, ROWS, SL), BF16),
        pltpu.SemaphoreType.DMA((32,)),
        pltpu.SemaphoreType.DMA((N_SEND,)), pltpu.SemaphoreType.DMA((N_RECV,)),
    ]
    operands = (
        tokens, delta_state, attn_gain.reshape(1, D), query_weight, key_weight, value_weight, decay_weight.T,
        beta_weight.T, decay_rate.reshape(1, 2), head_gain.reshape(1, HEAD), output_weight, ffn_gain.reshape(1, D), expert_ids.T,
        expert_logit.T, group_prob.reshape(1, ROWS), expert_gate.reshape(D, 128), expert_up.reshape(D, 128),
        expert_down.reshape(128, D), dense_gate, dense_up, dense_down, dense_mix.reshape(1, SL),
    )
    operands = [pltpu.with_memory_space_constraint(o, pltpu.HBM) for o in operands]
    mixed_out, new_state = pl.pallas_call(
        kernel,
        out_shape=(
            jax.ShapeDtypeStruct((ROWS, SL), BF16),
            jax.ShapeDtypeStruct((ROWS, 2, HEAD, HEAD), F32),
        ),
        in_specs=in_specs,
        out_specs=(pl.BlockSpec(memory_space=pltpu.VMEM), pl.BlockSpec(memory_space=pl.ANY)),
        scratch_shapes=scratch,
        compiler_params=pltpu.CompilerParams(
            collective_id=0, has_side_effects=True, vmem_limit_bytes=24 * 1024 * 1024),
        name="layer",
    )(*operands)
    return mixed_out, new_state


def solution(mesh):
    return jax.shard_map(
        per_device,
        mesh=mesh,
        in_specs=(
            P("ep", None),
            P("ep", "tp", None, None),
            P(),
            P("ep", "tp"),
            P("ep", "tp"),
            P("ep", "tp"),
            P(),
            P(),
            P("tp"),
            P(),
            P("tp", None),
            P(),
            P("ep", None),
            P("ep"),
            P("ep", None),
            P("ep", None, "tp"),
            P("ep", None, "tp"),
            P("ep", "tp", None),
            P("tp", "ep"),
            P("tp", "ep"),
            P("ep", "tp"),
            P("tp"),
        ),
        out_specs=(P("ep", "tp"), P("ep", "tp", None, None)),
        check_vma=False,
    )
```
